32 devices in a mesh: ep: 4 (over z), tp: 8 (over y, x, core).
Axes of the slice: x: 2, y: 2, z: 4, core: 2. Of those that a mesh axis runs over, the one named last changes fastest.
Arguments:
- tokens: bfloat16 [512, 2048], P('ep', 'tp'), may hold values from -6 to 6
- out_grad: bfloat16 [512, 2048], P('ep', 'tp'), may hold values from -6 to 6
- routes: int32 [512, 2], P('ep'), may hold values from 0 to 3, all different within a row; in each aligned block of 128 rows (0 to 127, 128 to 255, ...) at most 96 rows name the same one
- gates: float32 [512, 2], P('ep'), may hold values from 0.1 to 0.9
- gate_weight: bfloat16 [4, 2048, 5632], P('ep', None, 'tp'), may hold values from -0.125 to 0.125
- up_weight: bfloat16 [4, 2048, 5632], P('ep', None, 'tp'), may hold values from -0.125 to 0.125
- down_weight: bfloat16 [4, 5632, 2048], P('ep', 'tp'), may hold values from -0.078125 to 0.078125
Outputs:
- tokens_grad: bfloat16 [512, 2048], P('ep', 'tp')
- gates_grad: float32 [512, 2], P(('ep', 'tp'))
- gate_weight_grad: bfloat16 [4, 2048, 5632], P('ep', None, 'tp')
- up_weight_grad: bfloat16 [4, 2048, 5632], P('ep', None, 'tp')
- down_weight_grad: bfloat16 [4, 5632, 2048], P('ep', 'tp')
The draws below stay inside these ranges and needn't reach their ends.
Inputs may be any that keep to these rules, and one draw needn't show every extreme that they name: `routes`: the 2 experts of a token differ. In each aligned block of 128 rows (the tokens of one index of ep) no expert is named by more than 96 rows, a bound that some block reaches.
All inputs are finite; a program needn't handle non-finite values.
Results may differ from the reference program's by a relative error of at most 0.029.
Values may be sent and summed in bfloat16 or wider, within the bound.
A program may use at most 64 MiB of HBM per device.

```python
import math
import jax
import jax.numpy as jnp
import numpy as np
from jax import lax

D = 2048
FF = 5632
TOPK = 2
TOK_DEV = 128
EXPERTS = 4
CAP = 96
TOKENS = 512
N_EP = 4
N_TP = 8


def block_scale(stream_key, dims, split, least, top_value):
    gain = 1.0
    for dim, parts in split:
        steps = jax.random.uniform(jax.random.fold_in(jax.random.fold_in(stream_key, 6), dim), (parts,), jnp.float32, least / len(split), top_value / len(split))
        gain = gain * jnp.repeat(jnp.exp(steps), dims[dim] // parts).reshape((-1,) + (1,) * (len(dims) - 1 - dim))
    return gain


def routed_block(own_key, own, number, rows, count, top, reach, slope):
    ranking = jax.random.permutation(own_key, count)
    crowded, ordinary = portions_of(count, rows * top, reach, slope, True), portions_of(count, rows * top, reach, slope, False)
    places = jnp.arange(count)

    def named(tallies, rotation):
        used = int((tallies > 0).sum())
        fixed = max(1, used // 4)
        moved = fixed + (places - fixed + rotation * (used - fixed)) % max(1, count - fixed)
        return jnp.zeros((count,), jnp.int32).at[ranking[jnp.where(places < fixed, places, moved)]].set(jnp.asarray(tallies, jnp.int32))

    tallies = jnp.where(number % 4 == 0, named(crowded, number // 4), named(ordinary, number - number // 4 - 1))
    mixed = jax.random.permutation(jax.random.fold_in(own, 3), count)
    source_of, taker = mixed[0:count // 2 * 2:2], mixed[1:count // 2 * 2:2]
    room = jnp.minimum(tallies[source_of] - 1, reach - tallies[taker]) // 2
    room = jnp.where((source_of == ranking[0]) | (taker == ranking[0]) | (tallies[taker] == 0), 0, jnp.maximum(room, 0))
    moved = jax.random.randint(jax.random.fold_in(own, 4), (count // 2,), 0, 1 << 20) % (room + 1)
    tallies = tallies.at[source_of].add(-moved).at[taker].add(moved)
    items = jnp.searchsorted(jnp.cumsum(tallies), jnp.arange(rows * top), side="right").astype(jnp.int32)
    grid = items.reshape(top, rows).T
    grid = grid[jax.random.permutation(jax.random.fold_in(own, 1), rows)]
    rotation = jax.random.randint(jax.random.fold_in(own, 2), (rows, 1), 0, top)
    return jnp.take_along_axis(grid, (jnp.arange(top)[None, :] + rotation) % top, axis=1)


def portions_of(count, total, bound, slope, full):
    portions = [(1 << 20) // math.isqrt(rank ** slope) + 1 for rank in range(1, count + 1)]
    largest = bound if full else min(bound, max(-(-total // count), total * portions[0] // sum(portions)))
    least = 1 if total - largest >= count - 1 else 0
    holding, surplus = [largest] + [least] * (count - 1), total - largest - least * (count - 1)
    while surplus > 0:
        free = [i for i in range(1, count) if holding[i] < largest] or [i for i in range(1, count) if holding[i] < bound]
        pool, left = sum([portions[i] for i in free]), surplus
        for i in free:
            addition = min(bound - holding[i], max(1, left * portions[i] // pool), surplus)
            holding[i] = holding[i] + addition
            surplus = surplus - addition
    return np.array(holding)


def scatter_about(stream_key, extent, deviation, most, cuts=(), held_as=jnp.bfloat16):
    loudness = block_scale(stream_key, extent, cuts, -0.22, 0.18) if cuts else 1.0
    entries = jax.random.normal(stream_key, extent, jnp.float32) * deviation * loudness
    return jnp.minimum(jnp.maximum(entries, -most), most).astype(held_as)


def setup_inputs(seed: int = 0) -> dict:
    arg_keys = jax.random.split(jax.random.key(seed), 8)
    tokens = scatter_about(arg_keys[0], (TOKENS, D), 1.0, 6.0, ((0, 4), (1, 8)))
    out_grad = scatter_about(arg_keys[1], (TOKENS, D), 1.0, 6.0, ((0, 4), (1, 8)))
    routes_keys = jax.random.split(jax.random.fold_in(arg_keys[2], 1), TOKENS // TOK_DEV)
    routes_turns = jax.random.permutation(jax.random.fold_in(arg_keys[2], 3), TOKENS // TOK_DEV)
    routes = jax.vmap(lambda own, number: routed_block(jax.random.fold_in(arg_keys[2], 2), own, number, TOK_DEV, EXPERTS, TOPK, CAP, 2))(routes_keys, routes_turns).reshape((TOKENS, TOPK))
    gates = jnp.clip(0.1 + 0.79999997 * jax.random.uniform(arg_keys[3], (TOKENS, TOPK), jnp.float32) ** block_scale(arg_keys[3], (TOKENS, TOPK), ((0, 4),), -0.2, 0.2), 0.1, 0.9)
    gate_weight = scatter_about(arg_keys[4], (EXPERTS, D, FF), D ** -0.5, 0.125, ((0, 4), (2, 8)))
    up_weight = scatter_about(arg_keys[5], (EXPERTS, D, FF), D ** -0.5, 0.125, ((0, 4), (2, 8)))
    down_weight = scatter_about(arg_keys[6], (EXPERTS, FF, D), FF ** -0.5, 0.078125, ((0, 4), (1, 8)))
    return {"tokens": tokens, "out_grad": out_grad, "routes": routes, "gates": gates, "gate_weight": gate_weight, "up_weight": up_weight, "down_weight": down_weight}


def expert_grads(rows, cotan, w_gate, w_up, w_down):
    pre_gate = jnp.dot(rows, w_gate, preferred_element_type=jnp.float32)
    pre_up = jnp.dot(rows, w_up, preferred_element_type=jnp.float32)
    activated = jax.nn.silu(pre_gate)
    hidden = (activated * pre_up).astype(jnp.bfloat16)
    hid_grad = jnp.dot(cotan, w_down.T, preferred_element_type=jnp.float32)
    sigmoid_gate = jax.nn.sigmoid(pre_gate)
    gate_part = (hid_grad * pre_up * sigmoid_gate * (1.0 + pre_gate * (1.0 - sigmoid_gate))).astype(jnp.bfloat16)
    up_part = (hid_grad * activated).astype(jnp.bfloat16)
    slot_dots = jnp.sum(hidden.astype(jnp.float32) * hid_grad, axis=1)
    down_grad = jnp.dot(hidden.T, cotan, preferred_element_type=jnp.float32).astype(jnp.bfloat16)
    gate_grad = jnp.dot(rows.T, gate_part, preferred_element_type=jnp.float32).astype(jnp.bfloat16)
    up_grad = jnp.dot(rows.T, up_part, preferred_element_type=jnp.float32).astype(jnp.bfloat16)
    return gate_part, up_part, slot_dots, gate_grad, up_grad, down_grad


def reference(tokens, out_grad, routes, gates, gate_weight, up_weight, down_weight):
    slot_count = TOKENS * TOPK
    flat = jnp.arange(slot_count, dtype=jnp.int32)
    token_of = (flat // TOPK).astype(jnp.int32)
    flat_expert = routes.reshape(-1).astype(jnp.int32)
    onehot = (flat_expert[:, None] == jnp.arange(EXPERTS, dtype=jnp.int32)[None, :]).astype(jnp.int32)
    blocks = onehot.reshape(N_EP, TOK_DEV * TOPK, EXPERTS)
    before = jnp.cumsum(blocks, axis=1) - blocks
    slot_rank = jnp.sum(before * blocks, axis=2).reshape(-1)
    source = (flat // (TOK_DEV * TOPK)).astype(jnp.int32)
    slot_dest = (flat_expert * (N_EP * CAP) + source * CAP + slot_rank).astype(jnp.int32)
    owner = jnp.full((EXPERTS * N_EP * CAP,), slot_count, jnp.int32).at[slot_dest].set(flat)
    owner = owner.reshape(EXPERTS, N_EP * CAP)
    zero_row = jnp.zeros((1, D), jnp.bfloat16)
    row_table = jnp.concatenate([tokens[token_of], zero_row], axis=0)
    scaled = (gates.reshape(-1)[:, None] * out_grad[token_of].astype(jnp.float32)).astype(jnp.bfloat16)
    cotan_table = jnp.concatenate([scaled, zero_row], axis=0)
    width = FF // N_TP

    def per_expert(inputs):
        index, w_gate, w_up, w_down = inputs
        rows = row_table[index]
        cotan = cotan_table[index]
        gate_part, up_part, slot_dots, gate_grad, up_grad, down_grad = expert_grads(rows, cotan, w_gate, w_up, w_down)
        count = index.shape[0]
        parts_gate = gate_part.reshape(count, N_TP, width).transpose(1, 0, 2)
        parts_up = up_part.reshape(count, N_TP, width).transpose(1, 0, 2)
        split_gate = w_gate.reshape(D, N_TP, width).transpose(1, 0, 2)
        split_up = w_up.reshape(D, N_TP, width).transpose(1, 0, 2)

        def add_slice(total, pieces):
            piece_gate, piece_up, weight_gate, weight_up = pieces
            term = jnp.dot(piece_gate, weight_gate.T, preferred_element_type=jnp.float32)
            term = term + jnp.dot(piece_up, weight_up.T, preferred_element_type=jnp.float32)
            rounded = lax.optimization_barrier(term.astype(jnp.bfloat16))
            return total + rounded.astype(jnp.float32), None

        row_grad, _ = lax.scan(add_slice, jnp.zeros((count, D), jnp.float32),
                               (parts_gate, parts_up, split_gate, split_up))
        return gate_grad, up_grad, down_grad, row_grad, slot_dots

    gate_grads, up_grads, down_grads, row_grads, dots = lax.map(
        per_expert, (owner, gate_weight, up_weight, down_weight))
    targets = owner.reshape(-1)
    slot_grad = jnp.zeros((slot_count + 1, D), jnp.float32).at[targets].add(row_grads.reshape(-1, D))
    tokens_grad = jnp.sum(slot_grad[:slot_count].reshape(TOKENS, TOPK, D), axis=1).astype(jnp.bfloat16)
    slot_dot = jnp.zeros((slot_count + 1,), jnp.float32).at[targets].add(dots.reshape(-1))
    gates_grad = slot_dot[:slot_count].reshape(TOKENS, TOPK) / gates
    return tokens_grad, gates_grad, gate_grads, up_grads, down_grads
```

```python
import functools

import jax
import jax.numpy as jnp
from jax import lax
from jax.experimental import pallas as pl
from jax.experimental.pallas import tpu as pltpu
from jax.sharding import PartitionSpec as P

MESH = pl.DeviceIdType.MESH
BF16 = jnp.bfloat16
F32 = jnp.float32
MIB = 1024 * 1024


def dot_nn(a, b):
    return lax.dot_general(a, b, (((1,), (0,)), ((), ())), preferred_element_type=F32)


def flip(t, bit):
    return t + bit - 2 * bit * lax.rem(lax.div(t, bit), 2)


def partner(t, mask):
    bit = 1
    while bit <= mask:
        if mask & bit:
            t = flip(t, bit)
        bit *= 2
    return t


def exchange_kernel(
    ep, tp, cap,
    tok_ref, og_ref, routes_ref, gates_ref, wg_hbm, wu_hbm, wd_hbm,
    tg_ref, gg_ref, ggo, ugo, dgo,
    wg, wu, wd, wgt, wut, wdt, sent, big, comb_ref, pick_ref,
    hid, gp, up, hid_t, gp_t, up_t, dcol,
    psib, rsib, own_sum, mine, pown, rown, tsum, back, dsend, drecv, dsum, dback,
    wsem,
    zs, zr, ns, nr, ds_, dr, ss, sr,
    bss, bsr, rs, rr, zbs, zbr, dts, dtr, dzs, dzr,
):
    me_e = lax.axis_index("ep")
    me_t = lax.axis_index("tp")
    core = lax.rem(me_t, 2)
    sib = flip(me_t, 1)
    nbr = (flip(me_t, 2), flip(me_t, 4))
    diag = flip(nbr[0], 4)
    slots = ep * cap
    tok_dev, dw = tok_ref.shape
    fw, model = wg.shape

    def rdma(src, dst, s_sem, r_sem, e, t):
        return pltpu.make_async_remote_copy(
            src_ref=src, dst_ref=dst, send_sem=s_sem, recv_sem=r_sem,
            device_id={"ep": e, "tp": t}, device_id_type=MESH,
        )

    loads = [
        pltpu.make_async_copy(src.at[0], dst, wsem.at[i])
        for i, (src, dst) in enumerate(((wg_hbm, wg), (wu_hbm, wu), (wd_hbm, wd)))
    ]
    for load in loads:
        load.start()

    barrier = pltpu.get_barrier_semaphore()
    for r in range(1, ep):
        pl.semaphore_signal(
            barrier, inc=1, device_id={"ep": partner(me_e, r), "tp": me_t}, device_id_type=MESH)
    for r in range(1, tp):
        pl.semaphore_signal(
            barrier, inc=1, device_id={"ep": me_e, "tp": partner(me_t, r)}, device_id_type=MESH)

    expert = [routes_ref[k : k + 1, :] for k in range(2)]
    place = [jnp.zeros((1, tok_dev), F32) for _ in range(2)]
    for k in range(2):
        for i in range(ep):
            place[k] = jnp.where(expert[k] == partner(me_e, i), float(i), place[k])
    group = lax.broadcasted_iota(jnp.int32, (16, tok_dev), 0).astype(F32)
    oh = [jnp.where(place[k] == group, 1.0, 0.0) for k in range(2)]
    row_id = lax.broadcasted_iota(jnp.int32, (tok_dev, tok_dev), 0)
    col_id = lax.broadcasted_iota(jnp.int32, (tok_dev, tok_dev), 1)
    above = jnp.where(row_id < col_id, 1.0, 0.0).astype(BF16)
    before = dot_nn((oh[0] + oh[1]).astype(BF16), above)
    rank = [
        jnp.sum(before * oh[0], axis=0, keepdims=True),
        jnp.sum((before + oh[0]) * oh[1], axis=0, keepdims=True),
    ]
    slot_id = lax.broadcasted_iota(jnp.int32, (slots, tok_dev), 0).astype(F32)
    slot_gate = jnp.zeros((slots, 1), F32)
    both = jnp.zeros((slots, tok_dev), F32)
    for k in range(2):
        pick = jnp.where(place[k] * float(cap) + rank[k] == slot_id, 1.0, 0.0)
        pick_ref[k] = pick
        both = both + pick
        slot_gate = slot_gate + jnp.sum(pick * gates_ref[k : k + 1, :], axis=1, keepdims=True)
    select = both.astype(BF16)
    sent[:, 0:dw] = dot_nn(select, tok_ref[...]).astype(BF16)
    sent[:, dw : 2 * dw] = (slot_gate * dot_nn(select, og_ref[...])).astype(BF16)
    big[me_t, 0:cap, :] = sent[0:cap, :]

    pl.semaphore_wait(barrier, ep - 1 + tp - 1)

    sends = []

    def start(copy):
        copy.start()
        sends.append(copy)
        return copy

    def rows_of(i):
        return pl.ds(i * cap, cap)

    halves = (pl.ds(0, dw), pl.ds(dw, dw))
    z_copy, n_copy, d_copy, s_copy = {}, {}, {}, {}

    for i in range(1, ep):
        z_copy[i] = start(rdma(
            sent.at[rows_of(i)], big.at[me_t, rows_of(i)], zs.at[i], zr.at[i], partner(me_e, i), me_t))

    def chunk(i, t):
        return big.at[t, rows_of(i)]

    def half(i, t, h):
        return big.at[t, rows_of(i), halves[h]]

    def to_sibling(i, kind, t):
        s_copy[i, kind] = start(rdma(
            chunk(i, t), chunk(i, t), ss.at[i * 4 + kind], sr.at[i * 4 + kind], me_e, sib))

    def stage_a(i):
        if i:
            z_copy[i].wait_recv()
        for d in range(2):
            n_copy[i, d] = start(rdma(
                chunk(i, me_t), chunk(i, me_t), ns.at[i * 2 + d], nr.at[i * 2 + d], me_e, nbr[d]))
        to_sibling(i, 0, me_t)

    def stage_b(i):
        for d in range(2):
            n_copy[i, d].wait_recv()
            d_copy[i, d] = start(rdma(
                half(i, nbr[d], d), half(i, nbr[d], d), ds_.at[i * 2 + d], dr.at[i * 2 + d], me_e, nbr[1 - d]))
            to_sibling(i, 1 + d, nbr[d])

    def stage_c(i):
        for d in range(2):
            d_copy[i, d].wait_recv()
        to_sibling(i, 3, diag)

    def settle(i):
        for kind in range(4):
            s_copy[i, kind].wait_recv()

    def turn(w, wt):
        @pl.loop(0, tp)
        def _(j):
            part = pl.ds(pl.multiple_of(j * dw, dw), dw)
            wt[part, :] = w[:, part].T

    lane = lax.broadcasted_iota(jnp.int32, (cap, 128), 1)

    def forward(i):
        at = rows_of(i)

        def product(h, wt):
            total = dot_nn(big[0, at, halves[h]], wt[0:dw, :])
            for j in range(1, tp):
                total = total + dot_nn(big[j, at, halves[h]], wt[j * dw : (j + 1) * dw, :])
            return total

        g, u, h = product(0, wgt), product(0, wut), product(1, wdt)
        sig = jax.nn.sigmoid(g)
        act = g * sig
        hidden = (act * u).astype(BF16)
        hid[at, :] = hidden
        gp[at, :] = (h * u * sig * (1.0 + g * (1.0 - sig))).astype(BF16)
        up[at, :] = (h * act).astype(BF16)
        dots = jnp.sum(hidden.astype(F32) * h, axis=1, keepdims=True)
        dcol[0:cap, :] = jnp.where(lane == i, dots, dcol[0:cap, :])

    chips = (diag, nbr[0], nbr[1], me_t)
    b_copy, r_copy = {}, {}

    def pieces(i):
        at = rows_of(i)
        for q in range(4):
            wide = pl.ds(pl.multiple_of(lax.div(chips[q], 2) * (2 * dw), 2 * dw), 2 * dw)
            both = dot_nn(gp[at, :], wg[:, wide]) + dot_nn(up[at, :], wu[:, wide])
            low, high = both[:, 0:dw], both[:, dw : 2 * dw]
            psib[i, q] = jnp.where(core == 0, high, low).astype(BF16)
            own = jnp.where(core == 0, low, high)
            if q < 3:
                own_sum[i, q] = own
            else:
                mine[i] = own
            b_copy[i, q] = start(rdma(
                psib.at[i, q], rsib.at[i, q], bss.at[i * 4 + q], bsr.at[i * 4 + q], me_e, sib))

    def spread(i):
        for q in range(3):
            b_copy[i, q].wait_recv()
            pown[i, q] = (own_sum[i, q] + rsib[i, q].astype(F32)).astype(BF16)
            r_copy[i, q] = start(rdma(
                pown.at[i, q], rown.at[i, q], rs.at[i * 3 + q], rr.at[i * 3 + q], me_e, chips[q]))

    zb_copy = []

    def collect(i):
        b_copy[i, 3].wait_recv()
        total = mine[i] + rsib[i, 3].astype(F32)
        for q in range(3):
            r_copy[i, q].wait_recv()
            total = total + rown[i, q].astype(F32)
        if i:
            tsum[rows_of(i), :] = total.astype(BF16)
            zb_copy.append(start(rdma(
                tsum.at[rows_of(i)], back.at[rows_of(i)], zbs.at[i], zbr.at[i], partner(me_e, i), me_t)))
        else:
            back[rows_of(i), :] = total.astype(BF16)

    t_copy, dz_copy = [], []

    def send_dots():
        dsend[...] = dcol[...].T[0:8, :]
        for r in range(1, tp):
            t_copy.append(start(rdma(
                dsend, drecv.at[r - 1], dts.at[r - 1], dtr.at[r - 1], me_e, partner(me_t, r))))

    def return_dots():
        dots = dsend[...]
        for r in range(1, tp):
            t_copy[r - 1].wait_recv()
            dots = dots + drecv[r - 1]
        dsum[...] = dots
        for i in range(1, ep):
            dz_copy.append(start(rdma(
                dsum, dback.at[i], dzs.at[i], dzr.at[i], partner(me_e, i), me_t)))
        dback[0] = dots

    def weight_grad(rows_t, h, out):
        @pl.loop(0, tp)
        def _(j):
            part = pl.ds(pl.multiple_of(j * dw, dw), dw)
            out[:, part] = dot_nn(rows_t[...], big[j, :, halves[h]]).astype(BF16)

    dcol[...] = jnp.zeros_like(dcol)
    comb_ref[...] = both.T.astype(BF16)
    stage_a(0)
    loads[0].wait()
    turn(wg, wgt)
    loads[1].wait()
    turn(wu, wut)
    loads[2].wait()
    turn(wd, wdt)
    stage_b(0)
    stage_a(1)
    stage_c(0)
    if ep > 2:
        stage_a(2)
    settle(0)
    forward(0)
    stage_b(1)
    pieces(0)
    if ep > 2:
        stage_a(3)
        stage_b(2)
    stage_c(1)
    spread(0)
    settle(1)
    forward(1)
    if ep > 2:
        stage_b(3)
        pieces(1)
        stage_c(2)
        settle(2)
        forward(2)
        spread(1)
        collect(0)
        pieces(2)
        stage_c(3)
        spread(2)
        settle(3)
        forward(3)
        collect(1)
        send_dots()
        pieces(3)
        collect(2)
        hid_t[...] = hid[...].T
        gp_t[...] = gp[...].T
        up_t[...] = up[...].T
        spread(3)
        return_dots()
    else:
        send_dots()
        pieces(1)
        collect(0)
        hid_t[...] = hid[...].T
        gp_t[...] = gp[...].T
        up_t[...] = up[...].T
        spread(1)
        return_dots()
    weight_grad(gp_t, 0, ggo)
    collect(ep - 1)
    weight_grad(up_t, 0, ugo)
    weight_grad(hid_t, 1, dgo)

    for copy in dz_copy:
        copy.wait_recv()
    share = tok_dev // tp
    own_row = lax.broadcasted_iota(jnp.int32, (tok_dev, share), 0)
    own_col = lax.broadcasted_iota(jnp.int32, (tok_dev, share), 1) + me_t * share
    own_pick = jnp.where(own_row == own_col, 1.0, 0.0)
    tile_row = lax.broadcasted_iota(jnp.int32, (8, 128), 0)
    held = jnp.zeros((8, 128), F32)
    for i in range(ep):
        held = jnp.where(tile_row == i, dback[i], held)
    held = jnp.concatenate([held, jnp.zeros((120, 128), F32)], axis=0).T
    grads = []
    for k in range(2):
        total = jnp.zeros((1, tok_dev), F32)
        for i in range(ep):
            total = total + jnp.sum(
                held[0:cap, i : i + 1] * pick_ref[k, i * cap : (i + 1) * cap, :], axis=0, keepdims=True)
        grads.append(total / gates_ref[k : k + 1, :])
    shares = jnp.concatenate([*grads, jnp.zeros((6, tok_dev), F32)], axis=0)
    gg_ref[...] = jnp.dot(shares, own_pick, precision=lax.Precision.HIGHEST, preferred_element_type=F32)[0:2, :]

    for copy in zb_copy:
        copy.wait_recv()
    tg_ref[...] = dot_nn(comb_ref[...], back[...]).astype(BF16)
    for copy in sends:
        copy.wait_send()


def store_kernel(tg_ref, gg_ref, gw_ref, uw_ref, dw_ref, tg_out, gg_out, gw_out, uw_out, dw_out, sem):
    copies = [
        pltpu.make_async_copy(src, dst, sem.at[k])
        for k, (src, dst) in enumerate((
            (gw_ref, gw_out.at[0]), (uw_ref, uw_out.at[0]), (dw_ref, dw_out.at[0]),
            (tg_ref, tg_out), (gg_ref, gg_out)))
    ]
    for copy in copies:
        copy.start()
    for copy in copies:
        copy.wait()


def fused(tokens, out_grad, routes, gates, gate_weight, up_weight, down_weight):
    tok_dev, top_k = routes.shape
    ep = lax.axis_size("ep")
    tp = lax.axis_size("tp")
    cap = (3 * tok_dev + ep - 1) // ep
    slots = ep * cap
    dw = tokens.shape[1]
    model = gate_weight.shape[1]
    fw = gate_weight.shape[2]
    share = tok_dev // tp
    vmem = pl.BlockSpec(memory_space=pltpu.VMEM)
    any_ = pl.BlockSpec(memory_space=pl.ANY)
    dma = lambda n: pltpu.SemaphoreType.DMA((n,))
    flops = 16 * slots * model * fw
    small = (((tok_dev, dw), BF16), ((top_k, share), F32))
    grads = (((fw, model), BF16),) * 3
    results = pl.pallas_call(
        functools.partial(exchange_kernel, ep, tp, cap),
        out_shape=tuple(pltpu.VMEM(*leaf) for leaf in small + grads),
        in_specs=[vmem] * 4 + [any_] * 3,
        out_specs=[vmem] * 5,
        scratch_shapes=[
            pltpu.VMEM((fw, model), BF16),
            pltpu.VMEM((fw, model), BF16),
            pltpu.VMEM((fw, model), BF16),
            pltpu.VMEM((model, fw), BF16),
            pltpu.VMEM((model, fw), BF16),
            pltpu.VMEM((model, fw), BF16),
            pltpu.VMEM((slots, 2 * dw), BF16),
            pltpu.VMEM((tp, slots, 2 * dw), BF16),
            pltpu.VMEM((tok_dev, slots), BF16),
            pltpu.VMEM((2, slots, tok_dev), F32),
            pltpu.VMEM((slots, fw), BF16),
            pltpu.VMEM((slots, fw), BF16),
            pltpu.VMEM((slots, fw), BF16),
            pltpu.VMEM((fw, slots), BF16),
            pltpu.VMEM((fw, slots), BF16),
            pltpu.VMEM((fw, slots), BF16),
            pltpu.VMEM((128, 128), F32),
            pltpu.VMEM((ep, 4, cap, dw), BF16),
            pltpu.VMEM((ep, 4, cap, dw), BF16),
            pltpu.VMEM((ep, 3, cap, dw), F32),
            pltpu.VMEM((ep, cap, dw), F32),
            pltpu.VMEM((ep, 3, cap, dw), BF16),
            pltpu.VMEM((ep, 3, cap, dw), BF16),
            pltpu.VMEM((slots, dw), BF16),
            pltpu.VMEM((slots, dw), BF16),
            pltpu.VMEM((8, 128), F32),
            pltpu.VMEM((tp - 1, 8, 128), F32),
            pltpu.VMEM((8, 128), F32),
            pltpu.VMEM((ep, 8, 128), F32),
            dma(3),
            dma(ep), dma(ep), dma(2 * ep), dma(2 * ep), dma(2 * ep), dma(2 * ep),
            dma(4 * ep), dma(4 * ep),
            dma(4 * ep), dma(4 * ep), dma(3 * ep), dma(3 * ep), dma(ep), dma(ep),
            dma(tp), dma(tp), dma(ep), dma(ep),
        ],
        compiler_params=pltpu.CompilerParams(
            collective_id=0, has_side_effects=True, vmem_limit_bytes=46 * MIB),
        cost_estimate=pl.CostEstimate(flops=flops, bytes_accessed=6 * model * fw, transcendentals=0),
    )(tokens, out_grad, routes.T, gates.T, jnp.swapaxes(gate_weight, 1, 2),
      jnp.swapaxes(up_weight, 1, 2), down_weight)
    held = [pltpu.with_memory_space_constraint(r, pltpu.VMEM) for r in results]
    tokens_grad, gates_grad, gate_grad, up_grad, down_grad = pl.pallas_call(
        store_kernel,
        out_shape=tuple(jax.ShapeDtypeStruct(*leaf) for leaf in small)
        + tuple(jax.ShapeDtypeStruct((1, *shape), dtype) for shape, dtype in grads),
        in_specs=[vmem] * 5,
        out_specs=[any_] * 5,
        scratch_shapes=[dma(5)],
        compiler_params=pltpu.CompilerParams(vmem_limit_bytes=16 * MIB),
        cost_estimate=pl.CostEstimate(flops=slots * fw, bytes_accessed=6 * model * fw, transcendentals=0),
    )(*held)
    return (tokens_grad, gates_grad.T, jnp.swapaxes(gate_grad, 1, 2), jnp.swapaxes(up_grad, 1, 2), down_grad)


def fits_fused(ep, tp, tokens, routes, gate_weight):
    cap = (3 * routes.shape[0] + ep - 1) // ep
    return (
        tp == 8 and ep in (2, 4) and cap % 16 == 0 and cap <= 128
        and tokens.shape[1] % 128 == 0 and routes.shape[1] == 2
        and routes.shape[0] == 128
        and gate_weight.shape[2] % 16 == 0
    )


def expert_grads(rows, cotan, w_gate, w_up, w_down):
    pre_gate = jnp.dot(rows, w_gate, preferred_element_type=jnp.float32)
    pre_up = jnp.dot(rows, w_up, preferred_element_type=jnp.float32)
    activated = jax.nn.silu(pre_gate)
    hidden = (activated * pre_up).astype(jnp.bfloat16)
    hid_grad = jnp.dot(cotan, w_down.T, preferred_element_type=jnp.float32)
    sigmoid_gate = jax.nn.sigmoid(pre_gate)
    gate_part = (hid_grad * pre_up * sigmoid_gate * (1.0 + pre_gate * (1.0 - sigmoid_gate))).astype(
        jnp.bfloat16
    )
    up_part = (hid_grad * activated).astype(jnp.bfloat16)
    slot_dots = jnp.sum(hidden.astype(jnp.float32) * hid_grad, axis=1)
    down_grad = jnp.dot(hidden.T, cotan, preferred_element_type=jnp.float32).astype(jnp.bfloat16)
    gate_grad = jnp.dot(rows.T, gate_part, preferred_element_type=jnp.float32).astype(jnp.bfloat16)
    up_grad = jnp.dot(rows.T, up_part, preferred_element_type=jnp.float32).astype(jnp.bfloat16)
    return (gate_part, up_part, slot_dots, gate_grad, up_grad, down_grad)


def on_device(tokens, out_grad, routes, gates, gate_weight, up_weight, down_weight):
    tok_dev, top_k = routes.shape
    ep_size = lax.axis_size("ep")
    tp_size = lax.axis_size("tp")
    if fits_fused(ep_size, tp_size, tokens, routes, gate_weight):
        return fused(tokens, out_grad, routes, gates, gate_weight, up_weight, down_weight)
    capacity = (3 * tok_dev + ep_size - 1) // ep_size
    buffer_rows = ep_size * capacity
    slice_width = tokens.shape[1]
    flat_expert = routes.reshape(-1)
    onehot = (flat_expert[:, None] == jnp.arange(ep_size, dtype=jnp.int32)[None, :]).astype(
        jnp.int32
    )
    slot_rank = jnp.sum((jnp.cumsum(onehot, axis=0) - onehot) * onehot, axis=1)
    slot_dest = flat_expert * capacity + slot_rank
    placed = jnp.arange(buffer_rows, dtype=jnp.int32)[:, None] == slot_dest[None, :]
    placed_float = placed.astype(jnp.float32)
    select = jnp.any(placed.reshape(buffer_rows, tok_dev, top_k), axis=2).astype(jnp.bfloat16)
    slot_gate = jnp.dot(placed_float, gates.reshape(-1), precision=lax.Precision.HIGHEST)
    sent_rows = jnp.dot(select, tokens, preferred_element_type=jnp.float32).astype(jnp.bfloat16)
    cotan_rows = jnp.dot(select, out_grad, preferred_element_type=jnp.float32)
    sent_cotan = (slot_gate[:, None] * cotan_rows).astype(jnp.bfloat16)
    recv_rows, recv_cotan = (
        lax.all_to_all(
            sent_rows.reshape(ep_size, capacity, slice_width),
            "ep",
            split_axis=0,
            concat_axis=0,
            tiled=True,
        ),
        lax.all_to_all(
            sent_cotan.reshape(ep_size, capacity, slice_width),
            "ep",
            split_axis=0,
            concat_axis=0,
            tiled=True,
        ),
    )
    whole_rows, whole_cotan = (
        lax.all_gather(recv_rows, "tp", axis=2, tiled=True),
        lax.all_gather(recv_cotan, "tp", axis=2, tiled=True),
    )
    model_width = whole_rows.shape[2]
    rows = whole_rows.reshape(buffer_rows, model_width)
    cotan = whole_cotan.reshape(buffer_rows, model_width)
    w_gate = gate_weight[0]
    w_up = up_weight[0]
    gate_part, up_part, slot_dots, gate_grad, up_grad, down_grad = expert_grads(
        rows, cotan, w_gate, w_up, down_weight[0]
    )
    partial_value = jnp.dot(gate_part, w_gate.T, preferred_element_type=jnp.float32)
    partial_value = (
        partial_value + jnp.dot(up_part, w_up.T, preferred_element_type=jnp.float32)
    ).astype(jnp.bfloat16)
    share = tok_dev // tp_size
    start = lax.axis_index("tp") * share
    summed = lax.psum(slot_dots, "tp")
    row_sums = lax.psum_scatter(
        partial_value.reshape(ep_size, capacity, model_width), "tp", scatter_dimension=2, tiled=True
    ).astype(jnp.float32)
    back_rows, back_dots = (
        lax.all_to_all(
            row_sums.astype(jnp.bfloat16), "ep", split_axis=0, concat_axis=0, tiled=True
        ).astype(row_sums.dtype),
        lax.all_to_all(
            summed.reshape(ep_size, capacity).astype(jnp.bfloat16),
            "ep",
            split_axis=0,
            concat_axis=0,
            tiled=True,
        ).astype(jnp.float32),
    )
    slot_rows = back_rows.reshape(buffer_rows, slice_width)[slot_dest]
    tokens_grad = jnp.sum(slot_rows.reshape(tok_dev, top_k, slice_width), axis=1).astype(
        jnp.bfloat16
    )
    token_dots = back_dots.reshape(buffer_rows)[slot_dest].reshape(tok_dev, top_k)
    own_dots = lax.dynamic_slice_in_dim(token_dots, start, share, 0)
    own_gates = lax.dynamic_slice_in_dim(gates, start, share, 0)
    gates_grad = own_dots / own_gates
    return (tokens_grad, gates_grad, gate_grad[None], up_grad[None], down_grad[None])


def solution(mesh):
    placed = (
        P("ep", "tp"),
        P("ep", "tp"),
        P("ep", None),
        P("ep", None),
        P("ep", None, "tp"),
        P("ep", None, "tp"),
        P("ep", "tp", None),
    )
    return jax.shard_map(
        on_device,
        mesh=mesh,
        in_specs=placed,
        out_specs=(
            P("ep", "tp"),
            P(("ep", "tp"), None),
            P("ep", None, "tp"),
            P("ep", None, "tp"),
            P("ep", "tp", None),
        ),
        check_vma=False,
    )
```

```python
import functools

import jax
import jax.numpy as jnp
from jax import lax
from jax.experimental import pallas as pl
from jax.experimental.pallas import tpu as pltpu
from jax.sharding import PartitionSpec as P

MESH = pl.DeviceIdType.MESH
BF16 = jnp.bfloat16
F32 = jnp.float32
MIB = 1024 * 1024


def dot_nn(a, b):
    return lax.dot_general(a, b, (((1,), (0,)), ((), ())), preferred_element_type=F32)


def flip(t, bit):
    return t + bit - 2 * bit * lax.rem(lax.div(t, bit), 2)


def partner(t, mask):
    bit = 1
    while bit <= mask:
        if mask & bit:
            t = flip(t, bit)
        bit *= 2
    return t


def exchange_kernel(
    ep, tp, cap,
    tok_ref, og_ref, routes_ref, gates_ref, wg_hbm, wu_hbm, wd_hbm,
    tg_ref, gg_ref, ggo, ugo, dgo,
    wg, wu, wd, wgt, wut, wdt, sent, big, comb_ref, pick_ref,
    pg, pu, hid, gp, up, hid_t, gp_t, up_t, dcol,
    psib, rsib, own_sum, pown, rown, tsum, back, dsend, drecv, dsum, dback,
    wsem, out_sem, zr, nr, dr, sr, br, rr, zbr, dtr, dzr,
):
    me_e = lax.axis_index("ep")
    me_t = lax.axis_index("tp")
    core = lax.rem(me_t, 2)
    sib = flip(me_t, 1)
    nbr = (flip(me_t, 2), flip(me_t, 4))
    diag = flip(nbr[0], 4)
    slots = ep * cap
    tok_dev, dw = tok_ref.shape
    fw, model = wg.shape

    def rdma(src, dst, sem, e, t):
        return pltpu.make_async_remote_copy(
            src_ref=src, dst_ref=dst, send_sem=out_sem.at[0], recv_sem=sem,
            device_id={"ep": e, "tp": t}, device_id_type=MESH,
        )

    def arrived(ref, sem):
        rdma(ref, ref, sem, me_e, sib).wait_recv()

    loads = [
        pltpu.make_async_copy(src.at[0], dst, wsem.at[i])
        for i, (src, dst) in enumerate(((wg_hbm, wg), (wu_hbm, wu), (wd_hbm, wd)))
    ]
    for load in loads:
        load.start()

    barrier = pltpu.get_barrier_semaphore()
    for r in range(1, ep):
        pl.semaphore_signal(
            barrier, inc=1, device_id={"ep": partner(me_e, r), "tp": me_t}, device_id_type=MESH)
    for r in range(1, tp):
        pl.semaphore_signal(
            barrier, inc=1, device_id={"ep": me_e, "tp": partner(me_t, r)}, device_id_type=MESH)

    expert = [routes_ref[k : k + 1, :] for k in range(2)]
    place = [jnp.zeros((1, tok_dev), F32) for _ in range(2)]
    for k in range(2):
        for i in range(ep):
            place[k] = jnp.where(expert[k] == partner(me_e, i), float(i), place[k])
    group = lax.broadcasted_iota(jnp.int32, (16, tok_dev), 0).astype(F32)
    oh = [jnp.where(place[k] == group, 1.0, 0.0) for k in range(2)]
    row_id = lax.broadcasted_iota(jnp.int32, (tok_dev, tok_dev), 0)
    col_id = lax.broadcasted_iota(jnp.int32, (tok_dev, tok_dev), 1)
    above = jnp.where(row_id < col_id, 1.0, 0.0).astype(BF16)
    before = dot_nn((oh[0] + oh[1]).astype(BF16), above)
    rank = [
        jnp.sum(before * oh[0], axis=0, keepdims=True),
        jnp.sum((before + oh[0]) * oh[1], axis=0, keepdims=True),
    ]
    slot_id = lax.broadcasted_iota(jnp.int32, (slots, tok_dev), 0).astype(F32)
    slot_gate = jnp.zeros((slots, 1), F32)
    both = jnp.zeros((slots, tok_dev), F32)
    for k in range(2):
        pick = jnp.where(place[k] * float(cap) + rank[k] == slot_id, 1.0, 0.0)
        pick_ref[k] = pick
        both = both + pick
        slot_gate = slot_gate + jnp.sum(pick * gates_ref[k : k + 1, :], axis=1, keepdims=True)
    select = both.astype(BF16)
    sent[:, 0:dw] = dot_nn(select, tok_ref[...]).astype(BF16)
    sent[:, dw : 2 * dw] = (slot_gate * dot_nn(select, og_ref[...])).astype(BF16)
    big[me_t, 0:cap, :] = sent[0:cap, :]

    pl.semaphore_wait(barrier, ep - 1 + tp - 1)

    sends = []

    def send(src, dst, sem, e, t):
        copy = rdma(src, dst, sem, e, t)
        copy.start()
        sends.append(copy)

    def rows_of(i):
        return pl.ds(i * cap, cap)

    halves = (pl.ds(0, dw), pl.ds(dw, dw))
    direct = ()

    def chunk(i, t):
        return big.at[t, rows_of(i)]

    def half(i, t, h):
        return big.at[t, rows_of(i), halves[h]]

    def to_sibling(i, t):
        send(chunk(i, t), chunk(i, t), sr.at[i], me_e, sib)

    def send_z(i):
        return rdma(sent.at[rows_of(i)], big.at[me_t, rows_of(i)], zr.at[i], partner(me_e, i), me_t)

    def stage_a(i):
        if i:
            arrived(chunk(i, me_t), zr.at[i])
        for d in range(2):
            send(chunk(i, me_t), chunk(i, me_t), nr.at[2 * i + d], me_e, nbr[d])
        if i in direct:
            send(chunk(i, me_t), chunk(i, me_t), dr.at[i], me_e, diag)
        to_sibling(i, me_t)

    def stage_b(i):
        for d in range(2):
            arrived(chunk(i, nbr[d]), nr.at[2 * i + d])
            if i not in direct:
                send(half(i, nbr[d], d), half(i, nbr[d], d), dr.at[i], me_e, nbr[1 - d])
        for d in range(2):
            to_sibling(i, nbr[d])

    def stage_c(i):
        arrived(chunk(i, diag), dr.at[i])
        to_sibling(i, diag)

    def settle(i):
        arrived(big.at[pl.ds(0, 4), rows_of(i)], sr.at[i])

    def turn(w, wt):
        @pl.loop(0, tp)
        def _(j):
            part = pl.ds(pl.multiple_of(j * dw, dw), dw)
            wt[part, :] = w[:, part].T

    lane = lax.broadcasted_iota(jnp.int32, (cap, 128), 1)

    def product(i, h, wt):
        at = rows_of(i)
        total = dot_nn(big[0, at, halves[h]], wt[0:dw, :])
        for j in range(1, tp):
            total = total + dot_nn(big[j, at, halves[h]], wt[j * dw : (j + 1) * dw, :])
        return total

    def forward_x(i):
        pg[...] = product(i, 0, wgt)
        pu[...] = product(i, 0, wut)

    def forward_c(i):
        at = rows_of(i)
        g, u, h = pg[...], pu[...], product(i, 1, wdt)
        sig = jax.nn.sigmoid(g)
        act = g * sig
        hidden = (act * u).astype(BF16)
        hid[at, :] = hidden
        gp[at, :] = (h * u * sig * (1.0 + g * (1.0 - sig))).astype(BF16)
        up[at, :] = (h * act).astype(BF16)
        dots = jnp.sum(hidden.astype(F32) * h, axis=1, keepdims=True)
        dcol[0:cap, :] = jnp.where(lane == i, dots, dcol[0:cap, :])

    chips = (diag, nbr[0], nbr[1], me_t)

    def pieces(i):
        at = rows_of(i)
        for q in range(4):
            wide = pl.ds(pl.multiple_of(lax.div(chips[q], 2) * (2 * dw), 2 * dw), 2 * dw)
            both = dot_nn(gp[at, :], wg[:, wide]) + dot_nn(up[at, :], wu[:, wide])
            low, high = both[:, 0:dw], both[:, dw : 2 * dw]
            psib[i, q] = jnp.where(core == 0, high, low).astype(BF16)
            own_sum[i, q] = jnp.where(core == 0, low, high)
        send(psib.at[i], rsib.at[i], br.at[i], me_e, sib)

    def spread(i):
        arrived(rsib.at[i], br.at[i])
        for q in range(3):
            pown[i, q] = (own_sum[i, q] + rsib[i, q].astype(F32)).astype(BF16)
        for q in range(3):
            send(pown.at[i, q], rown.at[i, q], rr.at[i], me_e, chips[q])

    def collect(i):
        arrived(rown.at[i], rr.at[i])
        total = own_sum[i, 3] + rsib[i, 3].astype(F32)
        for q in range(3):
            total = total + rown[i, q].astype(F32)
        if i:
            tsum[rows_of(i), :] = total.astype(BF16)
            send(tsum.at[rows_of(i)], back.at[rows_of(i)], zbr.at[0], partner(me_e, i), me_t)
        else:
            back[rows_of(i), :] = total.astype(BF16)

    def send_dots():
        dsend[...] = dcol[...].T[0:8, :]
        for r in range(1, tp):
            send(dsend, drecv.at[r - 1], dtr.at[0], me_e, partner(me_t, r))

    def return_dots():
        arrived(drecv, dtr.at[0])
        dots = dsend[...]
        for r in range(1, tp):
            dots = dots + drecv[r - 1]
        dsum[...] = dots
        for i in range(1, ep):
            send(dsum, dback.at[i], dzr.at[0], partner(me_e, i), me_t)
        dback[0] = dots

    def weight_grad(rows_t, h, out, lo, hi):
        for k in range(lo, hi):
            out[:, k * dw : (k + 1) * dw] = dot_nn(rows_t[...], big[k, :, halves[h]]).astype(BF16)

    def flats():
        hid_t[...] = hid[...].T
        gp_t[...] = gp[...].T
        up_t[...] = up[...].T

    z_order = (1, 3, 2) if ep == 4 else (1,)
    z_sends = [send_z(i) for i in z_order]
    sends.extend(z_sends)
    for copy in z_sends:
        copy.start()
    stage_a(0)
    dcol[...] = jnp.zeros_like(dcol)
    comb_ref[...] = both.T.astype(BF16)
    for k, (w, wt) in enumerate(((wg, wgt), (wu, wut), (wd, wdt))):
        loads[k].wait()
        turn(w, wt)
    stage_b(0)
    stage_a(1)
    stage_c(0)
    settle(0)
    forward_x(0)
    stage_b(1)
    if ep == 4:
        forward_c(0)
        stage_a(3)
        pieces(0)
        stage_a(2)
        stage_c(1)
        settle(1)
        forward_x(1)
        stage_b(3)
        forward_c(1)
        stage_b(2)
        pieces(1)
        stage_c(3)
        settle(3)
        forward_x(3)
        spread(1)
        stage_c(2)
        forward_c(3)
        pieces(3)
        settle(2)
        forward_x(2)
        spread(3)
        forward_c(2)
        collect(1)
        send_dots()
        pieces(2)
        flats()
        weight_grad(gp_t, 0, ggo, 0, 4)
        spread(2)
        collect(3)
        return_dots()
        spread(0)
        weight_grad(gp_t, 0, ggo, 4, 8)
        weight_grad(up_t, 0, ugo, 0, 8)
        collect(2)
        weight_grad(hid_t, 1, dgo, 0, 4)
        collect(0)
        weight_grad(hid_t, 1, dgo, 4, 8)
    else:
        forward_c(0)
        stage_c(1)
        settle(1)
        forward_x(1)
        forward_c(1)
        send_dots()
        pieces(1)
        pieces(0)
        spread(1)
        flats()
        return_dots()
        spread(0)
        weight_grad(gp_t, 0, ggo, 0, 8)
        weight_grad(up_t, 0, ugo, 0, 8)
        collect(1)
        collect(0)
        weight_grad(hid_t, 1, dgo, 0, 8)

    arrived(dback.at[pl.ds(1, ep - 1)], dzr.at[0])
    share = tok_dev // tp
    own_row = lax.broadcasted_iota(jnp.int32, (tok_dev, share), 0)
    own_col = lax.broadcasted_iota(jnp.int32, (tok_dev, share), 1) + me_t * share
    own_pick = jnp.where(own_row == own_col, 1.0, 0.0)
    tile_row = lax.broadcasted_iota(jnp.int32, (8, 128), 0)
    held = jnp.zeros((8, 128), F32)
    for i in range(ep):
        held = jnp.where(tile_row == i, dback[i], held)
    held = jnp.concatenate([held, jnp.zeros((120, 128), F32)], axis=0).T
    grads = []
    for k in range(2):
        total = jnp.zeros((1, tok_dev), F32)
        for i in range(ep):
            total = total + jnp.sum(
                held[0:cap, i : i + 1] * pick_ref[k, i * cap : (i + 1) * cap, :], axis=0, keepdims=True)
        grads.append(total / gates_ref[k : k + 1, :])
    shares = jnp.concatenate([*grads, jnp.zeros((6, tok_dev), F32)], axis=0)
    gg_ref[...] = jnp.dot(shares, own_pick, precision=lax.Precision.HIGHEST, preferred_element_type=F32)[0:2, :]

    arrived(back.at[pl.ds(cap, slots - cap)], zbr.at[0])
    tg_ref[...] = dot_nn(comb_ref[...], back[...]).astype(BF16)
    for copy in sends:
        copy.wait_send()


def store_kernel(tg_ref, gg_ref, gw_ref, uw_ref, dw_ref, tg_out, gg_out, gw_out, uw_out, dw_out, sem):
    copies = [
        pltpu.make_async_copy(src, dst, sem.at[k])
        for k, (src, dst) in enumerate((
            (gw_ref, gw_out.at[0]), (uw_ref, uw_out.at[0]), (dw_ref, dw_out.at[0]),
            (tg_ref, tg_out), (gg_ref, gg_out)))
    ]
    for copy in copies:
        copy.start()
    for copy in copies:
        copy.wait()


def fused(tokens, out_grad, routes, gates, gate_weight, up_weight, down_weight):
    tok_dev, top_k = routes.shape
    ep = lax.axis_size("ep")
    tp = lax.axis_size("tp")
    cap = (3 * tok_dev + ep - 1) // ep
    slots = ep * cap
    dw = tokens.shape[1]
    model = gate_weight.shape[1]
    fw = gate_weight.shape[2]
    share = tok_dev // tp
    vmem = pl.BlockSpec(memory_space=pltpu.VMEM)
    any_ = pl.BlockSpec(memory_space=pl.ANY)
    dma = lambda n: pltpu.SemaphoreType.DMA((n,))
    flops = 16 * slots * model * fw
    small = (((tok_dev, dw), BF16), ((top_k, share), F32))
    grads = (((fw, model), BF16),) * 3
    results = pl.pallas_call(
        functools.partial(exchange_kernel, ep, tp, cap),
        out_shape=tuple(pltpu.VMEM(*leaf) for leaf in small + grads),
        in_specs=[vmem] * 4 + [any_] * 3,
        out_specs=[vmem] * 5,
        scratch_shapes=[
            pltpu.VMEM((fw, model), BF16),
            pltpu.VMEM((fw, model), BF16),
            pltpu.VMEM((fw, model), BF16),
            pltpu.VMEM((model, fw), BF16),
            pltpu.VMEM((model, fw), BF16),
            pltpu.VMEM((model, fw), BF16),
            pltpu.VMEM((slots, 2 * dw), BF16),
            pltpu.VMEM((tp, slots, 2 * dw), BF16),
            pltpu.VMEM((tok_dev, slots), BF16),
            pltpu.VMEM((2, slots, tok_dev), F32),
            pltpu.VMEM((cap, fw), F32),
            pltpu.VMEM((cap, fw), F32),
            pltpu.VMEM((slots, fw), BF16),
            pltpu.VMEM((slots, fw), BF16),
            pltpu.VMEM((slots, fw), BF16),
            pltpu.VMEM((fw, slots), BF16),
            pltpu.VMEM((fw, slots), BF16),
            pltpu.VMEM((fw, slots), BF16),
            pltpu.VMEM((128, 128), F32),
            pltpu.VMEM((ep, 4, cap, dw), BF16),
            pltpu.VMEM((ep, 4, cap, dw), BF16),
            pltpu.VMEM((ep, 4, cap, dw), F32),
            pltpu.VMEM((ep, 3, cap, dw), BF16),
            pltpu.VMEM((ep, 3, cap, dw), BF16),
            pltpu.VMEM((slots, dw), BF16),
            pltpu.VMEM((slots, dw), BF16),
            pltpu.VMEM((8, 128), F32),
            pltpu.VMEM((tp - 1, 8, 128), F32),
            pltpu.VMEM((8, 128), F32),
            pltpu.VMEM((ep, 8, 128), F32),
            dma(3), dma(1), dma(ep), dma(2 * ep), dma(ep), dma(ep), dma(ep), dma(ep), dma(1), dma(1), dma(1),
        ],
        compiler_params=pltpu.CompilerParams(
            collective_id=0, has_side_effects=True, vmem_limit_bytes=46 * MIB),
        cost_estimate=pl.CostEstimate(flops=flops, bytes_accessed=6 * model * fw, transcendentals=0),
    )(tokens, out_grad, routes.T, gates.T, jnp.swapaxes(gate_weight, 1, 2),
      jnp.swapaxes(up_weight, 1, 2), down_weight)
    held = [pltpu.with_memory_space_constraint(r, pltpu.VMEM) for r in results]
    tokens_grad, gates_grad, gate_grad, up_grad, down_grad = pl.pallas_call(
        store_kernel,
        out_shape=tuple(jax.ShapeDtypeStruct(*leaf) for leaf in small)
        + tuple(jax.ShapeDtypeStruct((1, *shape), dtype) for shape, dtype in grads),
        in_specs=[vmem] * 5,
        out_specs=[any_] * 5,
        scratch_shapes=[dma(5)],
        compiler_params=pltpu.CompilerParams(vmem_limit_bytes=16 * MIB),
        cost_estimate=pl.CostEstimate(flops=slots * fw, bytes_accessed=6 * model * fw, transcendentals=0),
    )(*held)
    return (tokens_grad, gates_grad.T, jnp.swapaxes(gate_grad, 1, 2), jnp.swapaxes(up_grad, 1, 2), down_grad)


def fits_fused(ep, tp, tokens, routes, gate_weight):
    cap = (3 * routes.shape[0] + ep - 1) // ep
    return (
        tp == 8 and ep in (2, 4) and cap % 16 == 0 and cap <= 128
        and tokens.shape[1] % 128 == 0 and routes.shape[1] == 2
        and routes.shape[0] == 128
        and gate_weight.shape[2] % 16 == 0
    )


def expert_grads(rows, cotan, w_gate, w_up, w_down):
    pre_gate = jnp.dot(rows, w_gate, preferred_element_type=jnp.float32)
    pre_up = jnp.dot(rows, w_up, preferred_element_type=jnp.float32)
    activated = jax.nn.silu(pre_gate)
    hidden = (activated * pre_up).astype(jnp.bfloat16)
    hid_grad = jnp.dot(cotan, w_down.T, preferred_element_type=jnp.float32)
    sigmoid_gate = jax.nn.sigmoid(pre_gate)
    gate_part = (hid_grad * pre_up * sigmoid_gate * (1.0 + pre_gate * (1.0 - sigmoid_gate))).astype(
        jnp.bfloat16
    )
    up_part = (hid_grad * activated).astype(jnp.bfloat16)
    slot_dots = jnp.sum(hidden.astype(jnp.float32) * hid_grad, axis=1)
    down_grad = jnp.dot(hidden.T, cotan, preferred_element_type=jnp.float32).astype(jnp.bfloat16)
    gate_grad = jnp.dot(rows.T, gate_part, preferred_element_type=jnp.float32).astype(jnp.bfloat16)
    up_grad = jnp.dot(rows.T, up_part, preferred_element_type=jnp.float32).astype(jnp.bfloat16)
    return (gate_part, up_part, slot_dots, gate_grad, up_grad, down_grad)


def on_device(tokens, out_grad, routes, gates, gate_weight, up_weight, down_weight):
    tok_dev, top_k = routes.shape
    ep_size = lax.axis_size("ep")
    tp_size = lax.axis_size("tp")
    if fits_fused(ep_size, tp_size, tokens, routes, gate_weight):
        return fused(tokens, out_grad, routes, gates, gate_weight, up_weight, down_weight)
    capacity = (3 * tok_dev + ep_size - 1) // ep_size
    buffer_rows = ep_size * capacity
    slice_width = tokens.shape[1]
    flat_expert = routes.reshape(-1)
    onehot = (flat_expert[:, None] == jnp.arange(ep_size, dtype=jnp.int32)[None, :]).astype(
        jnp.int32
    )
    slot_rank = jnp.sum((jnp.cumsum(onehot, axis=0) - onehot) * onehot, axis=1)
    slot_dest = flat_expert * capacity + slot_rank
    placed = jnp.arange(buffer_rows, dtype=jnp.int32)[:, None] == slot_dest[None, :]
    placed_float = placed.astype(jnp.float32)
    select = jnp.any(placed.reshape(buffer_rows, tok_dev, top_k), axis=2).astype(jnp.bfloat16)
    slot_gate = jnp.dot(placed_float, gates.reshape(-1), precision=lax.Precision.HIGHEST)
    sent_rows = jnp.dot(select, tokens, preferred_element_type=jnp.float32).astype(jnp.bfloat16)
    cotan_rows = jnp.dot(select, out_grad, preferred_element_type=jnp.float32)
    sent_cotan = (slot_gate[:, None] * cotan_rows).astype(jnp.bfloat16)
    recv_rows, recv_cotan = (
        lax.all_to_all(
            sent_rows.reshape(ep_size, capacity, slice_width),
            "ep",
            split_axis=0,
            concat_axis=0,
            tiled=True,
        ),
        lax.all_to_all(
            sent_cotan.reshape(ep_size, capacity, slice_width),
            "ep",
            split_axis=0,
            concat_axis=0,
            tiled=True,
        ),
    )
    whole_rows, whole_cotan = (
        lax.all_gather(recv_rows, "tp", axis=2, tiled=True),
        lax.all_gather(recv_cotan, "tp", axis=2, tiled=True),
    )
    model_width = whole_rows.shape[2]
    rows = whole_rows.reshape(buffer_rows, model_width)
    cotan = whole_cotan.reshape(buffer_rows, model_width)
    w_gate = gate_weight[0]
    w_up = up_weight[0]
    gate_part, up_part, slot_dots, gate_grad, up_grad, down_grad = expert_grads(
        rows, cotan, w_gate, w_up, down_weight[0]
    )
    partial_value = jnp.dot(gate_part, w_gate.T, preferred_element_type=jnp.float32)
    partial_value = (
        partial_value + jnp.dot(up_part, w_up.T, preferred_element_type=jnp.float32)
    ).astype(jnp.bfloat16)
    share = tok_dev // tp_size
    start = lax.axis_index("tp") * share
    summed = lax.psum(slot_dots, "tp")
    row_sums = lax.psum_scatter(
        partial_value.reshape(ep_size, capacity, model_width), "tp", scatter_dimension=2, tiled=True
    ).astype(jnp.float32)
    back_rows, back_dots = (
        lax.all_to_all(
            row_sums.astype(jnp.bfloat16), "ep", split_axis=0, concat_axis=0, tiled=True
        ).astype(row_sums.dtype),
        lax.all_to_all(
            summed.reshape(ep_size, capacity).astype(jnp.bfloat16),
            "ep",
            split_axis=0,
            concat_axis=0,
            tiled=True,
        ).astype(jnp.float32),
    )
    slot_rows = back_rows.reshape(buffer_rows, slice_width)[slot_dest]
    tokens_grad = jnp.sum(slot_rows.reshape(tok_dev, top_k, slice_width), axis=1).astype(
        jnp.bfloat16
    )
    token_dots = back_dots.reshape(buffer_rows)[slot_dest].reshape(tok_dev, top_k)
    own_dots = lax.dynamic_slice_in_dim(token_dots, start, share, 0)
    own_gates = lax.dynamic_slice_in_dim(gates, start, share, 0)
    gates_grad = own_dots / own_gates
    return (tokens_grad, gates_grad, gate_grad[None], up_grad[None], down_grad[None])


def solution(mesh):
    placed = (
        P("ep", "tp"),
        P("ep", "tp"),
        P("ep", None),
        P("ep", None),
        P("ep", None, "tp"),
        P("ep", None, "tp"),
        P("ep", "tp", None),
    )
    return jax.shard_map(
        on_device,
        mesh=mesh,
        in_specs=placed,
        out_specs=(
            P("ep", "tp"),
            P(("ep", "tp"), None),
            P("ep", None, "tp"),
            P("ep", None, "tp"),
            P("ep", "tp", None),
        ),
        check_vma=False,
    )
```

```python
import functools

import jax
import jax.numpy as jnp
from jax import lax
from jax.experimental import pallas as pl
from jax.experimental.pallas import tpu as pltpu
from jax.sharding import PartitionSpec as P

MESH = pl.DeviceIdType.MESH
BF16 = jnp.bfloat16
F32 = jnp.float32
MIB = 1024 * 1024


def dot_nn(a, b):
    return lax.dot_general(a, b, (((1,), (0,)), ((), ())), preferred_element_type=F32)


def flip(t, bit):
    return t + bit - 2 * bit * lax.rem(lax.div(t, bit), 2)


def partner(t, mask):
    bit = 1
    while bit <= mask:
        if mask & bit:
            t = flip(t, bit)
        bit *= 2
    return t


def exchange_kernel(
    ep, tp, cap,
    tok_hbm, og_hbm, routes_hbm, gates_hbm, wg_hbm, wu_hbm, wd_hbm,
    tg_ref, gg_ref, ggo, ugo, dgo,
    tok_ref, og_ref, routes_ref, gates_ref, wg, wu, wd, wgt, wut, wdt, sent, big, comb_ref, pick_ref,
    pg, pu, ph, hid, gp, up, hid_t, gp_t, up_t, dcol,
    psib, rsib, own_sum, pown, rown, tsum, back, dsend, drecv, dsum, dback,
    isem, wsem, out_sem, zr, nr, dr, sr, br, rr, zbr, dtr, dzr,
):
    me_e = lax.axis_index("ep")
    me_t = lax.axis_index("tp")
    core = lax.rem(me_t, 2)
    sib = flip(me_t, 1)
    nbr = (flip(me_t, 2), flip(me_t, 4))
    diag = flip(nbr[0], 4)
    slots = ep * cap
    tok_dev, dw = tok_ref.shape
    fw, model = wg.shape

    def rdma(src, dst, sem, e, t):
        return pltpu.make_async_remote_copy(
            src_ref=src, dst_ref=dst, send_sem=out_sem.at[0], recv_sem=sem,
            device_id={"ep": e, "tp": t}, device_id_type=MESH,
        )

    def arrived(ref, sem):
        rdma(ref, ref, sem, me_e, sib).wait_recv()

    inputs = [
        pltpu.make_async_copy(src, dst, isem.at[i])
        for i, (src, dst) in enumerate((
            (routes_hbm, routes_ref), (gates_hbm, gates_ref), (tok_hbm, tok_ref), (og_hbm, og_ref)))
    ]
    for load in inputs:
        load.start()
    loads = [
        pltpu.make_async_copy(src.at[0], dst, wsem.at[i])
        for i, (src, dst) in enumerate(((wg_hbm, wg), (wu_hbm, wu), (wd_hbm, wd)))
    ]
    barrier = pltpu.get_barrier_semaphore()
    for r in range(1, ep):
        pl.semaphore_signal(
            barrier, inc=1, device_id={"ep": partner(me_e, r), "tp": me_t}, device_id_type=MESH)
    for r in range(1, tp):
        pl.semaphore_signal(
            barrier, inc=1, device_id={"ep": me_e, "tp": partner(me_t, r)}, device_id_type=MESH)

    for load in loads:
        load.start()
    for load in inputs:
        load.wait()

    expert = [routes_ref[k : k + 1, :] for k in range(2)]
    place = [jnp.zeros((1, tok_dev), F32) for _ in range(2)]
    for k in range(2):
        for i in range(ep):
            place[k] = jnp.where(expert[k] == partner(me_e, i), float(i), place[k])
    group = lax.broadcasted_iota(jnp.int32, (16, tok_dev), 0).astype(F32)
    oh = [jnp.where(place[k] == group, 1.0, 0.0) for k in range(2)]
    row_id = lax.broadcasted_iota(jnp.int32, (tok_dev, tok_dev), 0)
    col_id = lax.broadcasted_iota(jnp.int32, (tok_dev, tok_dev), 1)
    above = jnp.where(row_id < col_id, 1.0, 0.0).astype(BF16)
    before = dot_nn((oh[0] + oh[1]).astype(BF16), above)
    rank = [
        jnp.sum(before * oh[0], axis=0, keepdims=True),
        jnp.sum((before + oh[0]) * oh[1], axis=0, keepdims=True),
    ]
    slot_id = lax.broadcasted_iota(jnp.int32, (slots, tok_dev), 0).astype(F32)
    slot_gate = jnp.zeros((slots, 1), F32)
    both = jnp.zeros((slots, tok_dev), F32)
    for k in range(2):
        pick = jnp.where(place[k] * float(cap) + rank[k] == slot_id, 1.0, 0.0)
        pick_ref[k] = pick
        both = both + pick
        slot_gate = slot_gate + jnp.sum(pick * gates_ref[k : k + 1, :], axis=1, keepdims=True)
    select = both.astype(BF16)
    sent[:, 0:dw] = dot_nn(select, tok_ref[...]).astype(BF16)
    sent[:, dw : 2 * dw] = (slot_gate * dot_nn(select, og_ref[...])).astype(BF16)
    big[me_t, 0:cap, :] = sent[0:cap, :]

    pl.semaphore_wait(barrier, ep - 1 + tp - 1)

    sends = []

    def send(src, dst, sem, e, t):
        copy = rdma(src, dst, sem, e, t)
        copy.start()
        sends.append(copy)

    def rows_of(i):
        return pl.ds(i * cap, cap)

    halves = (pl.ds(0, dw), pl.ds(dw, dw))
    direct = (1,)

    def chunk(i, t):
        return big.at[t, rows_of(i)]

    def half(i, t, h):
        return big.at[t, rows_of(i), halves[h]]

    def to_sibling(i, t, far=0):
        send(chunk(i, t), chunk(i, t), sr.at[2 * i + far], me_e, sib)

    def send_z(i):
        return rdma(sent.at[rows_of(i)], big.at[me_t, rows_of(i)], zr.at[i], partner(me_e, i), me_t)

    def stage_a(i):
        if i:
            arrived(chunk(i, me_t), zr.at[i])
        for d in range(2):
            send(chunk(i, me_t), chunk(i, me_t), nr.at[2 * i + d], me_e, nbr[d])
        if i in direct:
            send(chunk(i, me_t), chunk(i, me_t), dr.at[i], me_e, diag)
        to_sibling(i, me_t)

    def stage_b(i):
        for d in range(2):
            arrived(chunk(i, nbr[d]), nr.at[2 * i + d])
            if i not in direct:
                send(half(i, nbr[d], d), half(i, nbr[d], d), dr.at[i], me_e, nbr[1 - d])
        for d in range(2):
            to_sibling(i, nbr[d])

    def stage_c(i):
        arrived(chunk(i, diag), dr.at[i])
        to_sibling(i, diag, 1)

    def settle_near(i):
        arrived(big.at[pl.ds(0, 3), rows_of(i)], sr.at[2 * i])

    def settle_far(i):
        arrived(chunk(i, diag), sr.at[2 * i + 1])

    def turn(w, wt):
        @pl.loop(0, tp)
        def _(j):
            part = pl.ds(pl.multiple_of(j * dw, dw), dw)
            wt[part, :] = w[:, part].T

    lane = lax.broadcasted_iota(jnp.int32, (cap, 128), 1)

    chips = (diag, nbr[0], nbr[1], me_t)

    def product(i, h, wt, some):
        total = None
        for t in some:
            for k in range(2):
                j = lax.div(t, 2) * 2 + k
                term = dot_nn(big[j, rows_of(i), halves[h]], wt[pl.ds(pl.multiple_of(j * dw, dw), dw), :])
                total = term if total is None else total + term
        return total

    def near_x(i):
        pg[...] = product(i, 0, wgt, chips[1:])
        pu[...] = product(i, 0, wut, chips[1:])

    def near_c(i):
        ph[...] = product(i, 1, wdt, chips[1:])

    def forward(i):
        at = rows_of(i)
        g = pg[...] + product(i, 0, wgt, chips[:1])
        u = pu[...] + product(i, 0, wut, chips[:1])
        h = ph[...] + product(i, 1, wdt, chips[:1])
        sig = jax.nn.sigmoid(g)
        act = g * sig
        hidden = (act * u).astype(BF16)
        hid[at, :] = hidden
        gp[at, :] = (h * u * sig * (1.0 + g * (1.0 - sig))).astype(BF16)
        up[at, :] = (h * act).astype(BF16)
        dots = jnp.sum(hidden.astype(F32) * h, axis=1, keepdims=True)
        dcol[0:cap, :] = jnp.where(lane == i, dots, dcol[0:cap, :])

    def pieces(i, lo=0, hi=4):
        at = rows_of(i)
        for q in range(lo, hi):
            wide = pl.ds(pl.multiple_of(lax.div(chips[q], 2) * (2 * dw), 2 * dw), 2 * dw)
            both = dot_nn(gp[at, :], wg[:, wide]) + dot_nn(up[at, :], wu[:, wide])
            low, high = both[:, 0:dw], both[:, dw : 2 * dw]
            psib[i, q] = jnp.where(core == 0, high, low).astype(BF16)
            own_sum[i, q] = jnp.where(core == 0, low, high)
        part = pl.ds(lo, hi - lo)
        send(psib.at[i, part], rsib.at[i, part], br.at[2 * i + (lo > 0)], me_e, sib)

    def spread(i, lo=0, hi=4):
        arrived(rsib.at[i, pl.ds(lo, hi - lo)], br.at[2 * i + (lo > 0)])
        top = min(hi, 3)
        for q in range(lo, top):
            pown[i, q] = (own_sum[i, q] + rsib[i, q].astype(F32)).astype(BF16)
        for q in range(lo, top):
            send(pown.at[i, q], rown.at[i, q], rr.at[i], me_e, chips[q])

    def collect(i):
        arrived(rown.at[i], rr.at[i])
        total = own_sum[i, 3] + rsib[i, 3].astype(F32)
        for q in range(3):
            total = total + rown[i, q].astype(F32)
        if i:
            tsum[rows_of(i), :] = total.astype(BF16)
            send(tsum.at[rows_of(i)], back.at[rows_of(i)], zbr.at[i], partner(me_e, i), me_t)
        else:
            back[rows_of(i), :] = total.astype(BF16)

    def send_dots():
        dsend[...] = dcol[...].T[0:8, :]
        for r in range(1, tp):
            send(dsend, drecv.at[r - 1], dtr.at[0], me_e, partner(me_t, r))

    def return_dots():
        arrived(drecv, dtr.at[0])
        dots = dsend[...]
        for r in range(1, tp):
            dots = dots + drecv[r - 1]
        dsum[...] = dots
        for i in range(1, ep):
            send(dsum, dback.at[i], dzr.at[0], partner(me_e, i), me_t)
        dback[0] = dots

    def weight_grad(rows_t, h, out, lo, hi):
        for k in range(lo, hi):
            out[:, k * dw : (k + 1) * dw] = dot_nn(rows_t[...], big[k, :, halves[h]]).astype(BF16)

    def flats():
        hid_t[...] = hid[...].T
        gp_t[...] = gp[...].T
        up_t[...] = up[...].T

    z_order = (1, 3, 2) if ep == 4 else (1,)
    z_sends = [send_z(i) for i in z_order]
    sends.extend(z_sends)
    for copy in z_sends:
        copy.start()
    stage_a(0)
    dcol[...] = jnp.zeros_like(dcol)
    flat = both.T.astype(BF16)
    for i in range(ep):
        comb_ref[i] = flat[:, i * cap : (i + 1) * cap]
    for k, (w, wt) in enumerate(((wg, wgt), (wu, wut), (wd, wdt))):
        loads[k].wait()
        turn(w, wt)
    stage_b(0)
    stage_a(1)
    settle_near(0)
    near_x(0)
    near_c(0)
    stage_c(0)
    if ep == 4:
        stage_a(3)
        stage_b(1)
        stage_a(2)
        settle_far(0)
        forward(0)
        settle_near(1)
        near_x(1)
        stage_c(1)
        near_c(1)
        settle_far(1)
        forward(1)
        stage_b(3)
        pieces(1)
        stage_b(2)
        settle_near(3)
        near_x(3)
        near_c(3)
        stage_c(3)
        spread(1)
        pieces(0)
        settle_far(3)
        forward(3)
        stage_c(2)
        pieces(3)
        spread(0)
        settle_near(2)
        near_x(2)
        settle_far(2)
        spread(3)
        near_c(2)
        forward(2)
        send_dots()
        pieces(2, 0, 2)
        pieces(2, 2, 4)
        collect(1)
        flats()
        spread(2, 0, 2)
        weight_grad(gp_t, 0, ggo, 0, 2)
        spread(2, 2, 4)
        weight_grad(gp_t, 0, ggo, 2, 8)
        collect(3)
        return_dots()
        collect(0)
        weight_grad(up_t, 0, ugo, 0, 8)
        weight_grad(hid_t, 1, dgo, 0, 2)
        collect(2)
        weight_grad(hid_t, 1, dgo, 2, 8)
        last = 2
    else:
        stage_b(1)
        settle_far(0)
        forward(0)
        stage_c(1)
        settle_near(1)
        near_x(1)
        near_c(1)
        settle_far(1)
        forward(1)
        send_dots()
        pieces(1)
        pieces(0)
        spread(1)
        flats()
        return_dots()
        spread(0)
        weight_grad(gp_t, 0, ggo, 0, 8)
        weight_grad(up_t, 0, ugo, 0, 8)
        collect(1)
        collect(0)
        weight_grad(hid_t, 1, dgo, 0, 8)
        last = 1

    def token_part(i):
        if i:
            arrived(back.at[rows_of(i)], zbr.at[i])
        return dot_nn(comb_ref[i], back[rows_of(i), :])

    arrived(dback.at[pl.ds(1, ep - 1)], dzr.at[0])
    share = tok_dev // tp
    own_row = lax.broadcasted_iota(jnp.int32, (tok_dev, share), 0)
    own_col = lax.broadcasted_iota(jnp.int32, (tok_dev, share), 1) + me_t * share
    own_pick = jnp.where(own_row == own_col, 1.0, 0.0)
    tile_row = lax.broadcasted_iota(jnp.int32, (8, 128), 0)
    held = jnp.zeros((8, 128), F32)
    for i in range(ep):
        held = jnp.where(tile_row == i, dback[i], held)
    held = jnp.concatenate([held, jnp.zeros((120, 128), F32)], axis=0).T
    grads = []
    for k in range(2):
        total = jnp.zeros((1, tok_dev), F32)
        for i in range(ep):
            total = total + jnp.sum(
                held[0:cap, i : i + 1] * pick_ref[k, i * cap : (i + 1) * cap, :], axis=0, keepdims=True)
        grads.append(total / gates_ref[k : k + 1, :])
    shares = jnp.concatenate([*grads, jnp.zeros((6, tok_dev), F32)], axis=0)
    gg_ref[...] = jnp.dot(shares, own_pick, precision=lax.Precision.HIGHEST, preferred_element_type=F32)[0:2, :]

    total = token_part(0)
    for i in range(1, ep):
        if i != last:
            total = total + token_part(i)
    tg_ref[...] = (total + token_part(last)).astype(BF16)
    for copy in sends:
        copy.wait_send()


def store_kernel(tg_ref, gg_ref, gw_ref, uw_ref, dw_ref, tg_out, gg_out, gw_out, uw_out, dw_out, sem):
    copies = [
        pltpu.make_async_copy(src, dst, sem.at[k])
        for k, (src, dst) in enumerate((
            (gw_ref, gw_out.at[0]), (uw_ref, uw_out.at[0]), (dw_ref, dw_out.at[0]),
            (tg_ref, tg_out), (gg_ref, gg_out)))
    ]
    for copy in copies:
        copy.start()
    for copy in copies:
        copy.wait()


def fused(tokens, out_grad, routes, gates, gate_weight, up_weight, down_weight):
    tok_dev, top_k = routes.shape
    ep = lax.axis_size("ep")
    tp = lax.axis_size("tp")
    cap = (3 * tok_dev + ep - 1) // ep
    slots = ep * cap
    dw = tokens.shape[1]
    model = gate_weight.shape[1]
    fw = gate_weight.shape[2]
    share = tok_dev // tp
    vmem = pl.BlockSpec(memory_space=pltpu.VMEM)
    any_ = pl.BlockSpec(memory_space=pl.ANY)
    dma = lambda n: pltpu.SemaphoreType.DMA((n,))
    flops = 16 * slots * model * fw
    small = (((tok_dev, dw), BF16), ((top_k, share), F32))
    grads = (((fw, model), BF16),) * 3
    results = pl.pallas_call(
        functools.partial(exchange_kernel, ep, tp, cap),
        out_shape=tuple(pltpu.VMEM(*leaf) for leaf in small + grads),
        in_specs=[any_] * 7,
        out_specs=[vmem] * 5,
        scratch_shapes=[
            pltpu.VMEM((tok_dev, dw), BF16),
            pltpu.VMEM((tok_dev, dw), BF16),
            pltpu.VMEM((top_k, tok_dev), jnp.int32),
            pltpu.VMEM((top_k, tok_dev), F32),
            pltpu.VMEM((fw, model), BF16),
            pltpu.VMEM((fw, model), BF16),
            pltpu.VMEM((fw, model), BF16),
            pltpu.VMEM((model, fw), BF16),
            pltpu.VMEM((model, fw), BF16),
            pltpu.VMEM((model, fw), BF16),
            pltpu.VMEM((slots, 2 * dw), BF16),
            pltpu.VMEM((tp, slots, 2 * dw), BF16),
            pltpu.VMEM((ep, tok_dev, cap), BF16),
            pltpu.VMEM((2, slots, tok_dev), F32),
            pltpu.VMEM((cap, fw), F32),
            pltpu.VMEM((cap, fw), F32),
            pltpu.VMEM((cap, fw), F32),
            pltpu.VMEM((slots, fw), BF16),
            pltpu.VMEM((slots, fw), BF16),
            pltpu.VMEM((slots, fw), BF16),
            pltpu.VMEM((fw, slots), BF16),
            pltpu.VMEM((fw, slots), BF16),
            pltpu.VMEM((fw, slots), BF16),
            pltpu.VMEM((128, 128), F32),
            pltpu.VMEM((ep, 4, cap, dw), BF16),
            pltpu.VMEM((ep, 4, cap, dw), BF16),
            pltpu.VMEM((ep, 4, cap, dw), F32),
            pltpu.VMEM((ep, 3, cap, dw), BF16),
            pltpu.VMEM((ep, 3, cap, dw), BF16),
            pltpu.VMEM((slots, dw), BF16),
            pltpu.VMEM((slots, dw), BF16),
            pltpu.VMEM((8, 128), F32),
            pltpu.VMEM((tp - 1, 8, 128), F32),
            pltpu.VMEM((8, 128), F32),
            pltpu.VMEM((ep, 8, 128), F32),
            dma(4), dma(3), dma(1), dma(ep), dma(2 * ep), dma(ep), dma(2 * ep), dma(2 * ep), dma(ep), dma(ep),
            dma(1), dma(1),
        ],
        compiler_params=pltpu.CompilerParams(
            collective_id=0, has_side_effects=True, vmem_limit_bytes=46 * MIB),
        cost_estimate=pl.CostEstimate(flops=flops, bytes_accessed=6 * model * fw, transcendentals=0),
    )(tokens, out_grad, routes.T, gates.T, jnp.swapaxes(gate_weight, 1, 2),
      jnp.swapaxes(up_weight, 1, 2), down_weight)
    held = [pltpu.with_memory_space_constraint(r, pltpu.VMEM) for r in results]
    tokens_grad, gates_grad, gate_grad, up_grad, down_grad = pl.pallas_call(
        store_kernel,
        out_shape=tuple(jax.ShapeDtypeStruct(*leaf) for leaf in small)
        + tuple(jax.ShapeDtypeStruct((1, *shape), dtype) for shape, dtype in grads),
        in_specs=[vmem] * 5,
        out_specs=[any_] * 5,
        scratch_shapes=[dma(5)],
        compiler_params=pltpu.CompilerParams(vmem_limit_bytes=16 * MIB),
        cost_estimate=pl.CostEstimate(flops=slots * fw, bytes_accessed=6 * model * fw, transcendentals=0),
    )(*held)
    return (tokens_grad, gates_grad.T, jnp.swapaxes(gate_grad, 1, 2), jnp.swapaxes(up_grad, 1, 2), down_grad)


def fits_fused(ep, tp, tokens, routes, gate_weight):
    cap = (3 * routes.shape[0] + ep - 1) // ep
    return (
        tp == 8 and ep in (2, 4) and cap % 16 == 0 and cap <= 128
        and tokens.shape[1] % 128 == 0 and routes.shape[1] == 2
        and routes.shape[0] == 128
        and gate_weight.shape[2] % 16 == 0
    )


def expert_grads(rows, cotan, w_gate, w_up, w_down):
    pre_gate = jnp.dot(rows, w_gate, preferred_element_type=jnp.float32)
    pre_up = jnp.dot(rows, w_up, preferred_element_type=jnp.float32)
    activated = jax.nn.silu(pre_gate)
    hidden = (activated * pre_up).astype(jnp.bfloat16)
    hid_grad = jnp.dot(cotan, w_down.T, preferred_element_type=jnp.float32)
    sigmoid_gate = jax.nn.sigmoid(pre_gate)
    gate_part = (hid_grad * pre_up * sigmoid_gate * (1.0 + pre_gate * (1.0 - sigmoid_gate))).astype(
        jnp.bfloat16
    )
    up_part = (hid_grad * activated).astype(jnp.bfloat16)
    slot_dots = jnp.sum(hidden.astype(jnp.float32) * hid_grad, axis=1)
    down_grad = jnp.dot(hidden.T, cotan, preferred_element_type=jnp.float32).astype(jnp.bfloat16)
    gate_grad = jnp.dot(rows.T, gate_part, preferred_element_type=jnp.float32).astype(jnp.bfloat16)
    up_grad = jnp.dot(rows.T, up_part, preferred_element_type=jnp.float32).astype(jnp.bfloat16)
    return (gate_part, up_part, slot_dots, gate_grad, up_grad, down_grad)


def on_device(tokens, out_grad, routes, gates, gate_weight, up_weight, down_weight):
    tok_dev, top_k = routes.shape
    ep_size = lax.axis_size("ep")
    tp_size = lax.axis_size("tp")
    if fits_fused(ep_size, tp_size, tokens, routes, gate_weight):
        return fused(tokens, out_grad, routes, gates, gate_weight, up_weight, down_weight)
    capacity = (3 * tok_dev + ep_size - 1) // ep_size
    buffer_rows = ep_size * capacity
    slice_width = tokens.shape[1]
    flat_expert = routes.reshape(-1)
    onehot = (flat_expert[:, None] == jnp.arange(ep_size, dtype=jnp.int32)[None, :]).astype(
        jnp.int32
    )
    slot_rank = jnp.sum((jnp.cumsum(onehot, axis=0) - onehot) * onehot, axis=1)
    slot_dest = flat_expert * capacity + slot_rank
    placed = jnp.arange(buffer_rows, dtype=jnp.int32)[:, None] == slot_dest[None, :]
    placed_float = placed.astype(jnp.float32)
    select = jnp.any(placed.reshape(buffer_rows, tok_dev, top_k), axis=2).astype(jnp.bfloat16)
    slot_gate = jnp.dot(placed_float, gates.reshape(-1), precision=lax.Precision.HIGHEST)
    sent_rows = jnp.dot(select, tokens, preferred_element_type=jnp.float32).astype(jnp.bfloat16)
    cotan_rows = jnp.dot(select, out_grad, preferred_element_type=jnp.float32)
    sent_cotan = (slot_gate[:, None] * cotan_rows).astype(jnp.bfloat16)
    recv_rows, recv_cotan = (
        lax.all_to_all(
            sent_rows.reshape(ep_size, capacity, slice_width),
            "ep",
            split_axis=0,
            concat_axis=0,
            tiled=True,
        ),
        lax.all_to_all(
            sent_cotan.reshape(ep_size, capacity, slice_width),
            "ep",
            split_axis=0,
            concat_axis=0,
            tiled=True,
        ),
    )
    whole_rows, whole_cotan = (
        lax.all_gather(recv_rows, "tp", axis=2, tiled=True),
        lax.all_gather(recv_cotan, "tp", axis=2, tiled=True),
    )
    model_width = whole_rows.shape[2]
    rows = whole_rows.reshape(buffer_rows, model_width)
    cotan = whole_cotan.reshape(buffer_rows, model_width)
    w_gate = gate_weight[0]
    w_up = up_weight[0]
    gate_part, up_part, slot_dots, gate_grad, up_grad, down_grad = expert_grads(
        rows, cotan, w_gate, w_up, down_weight[0]
    )
    partial_value = jnp.dot(gate_part, w_gate.T, preferred_element_type=jnp.float32)
    partial_value = (
        partial_value + jnp.dot(up_part, w_up.T, preferred_element_type=jnp.float32)
    ).astype(jnp.bfloat16)
    share = tok_dev // tp_size
    start = lax.axis_index("tp") * share
    summed = lax.psum(slot_dots, "tp")
    row_sums = lax.psum_scatter(
        partial_value.reshape(ep_size, capacity, model_width), "tp", scatter_dimension=2, tiled=True
    ).astype(jnp.float32)
    back_rows, back_dots = (
        lax.all_to_all(
            row_sums.astype(jnp.bfloat16), "ep", split_axis=0, concat_axis=0, tiled=True
        ).astype(row_sums.dtype),
        lax.all_to_all(
            summed.reshape(ep_size, capacity).astype(jnp.bfloat16),
            "ep",
            split_axis=0,
            concat_axis=0,
            tiled=True,
        ).astype(jnp.float32),
    )
    slot_rows = back_rows.reshape(buffer_rows, slice_width)[slot_dest]
    tokens_grad = jnp.sum(slot_rows.reshape(tok_dev, top_k, slice_width), axis=1).astype(
        jnp.bfloat16
    )
    token_dots = back_dots.reshape(buffer_rows)[slot_dest].reshape(tok_dev, top_k)
    own_dots = lax.dynamic_slice_in_dim(token_dots, start, share, 0)
    own_gates = lax.dynamic_slice_in_dim(gates, start, share, 0)
    gates_grad = own_dots / own_gates
    return (tokens_grad, gates_grad, gate_grad[None], up_grad[None], down_grad[None])


def solution(mesh):
    placed = (
        P("ep", "tp"),
        P("ep", "tp"),
        P("ep", None),
        P("ep", None),
        P("ep", None, "tp"),
        P("ep", None, "tp"),
        P("ep", "tp", None),
    )
    return jax.shard_map(
        on_device,
        mesh=mesh,
        in_specs=placed,
        out_specs=(
            P("ep", "tp"),
            P(("ep", "tp"), None),
            P("ep", None, "tp"),
            P("ep", None, "tp"),
            P("ep", "tp", None),
        ),
        check_vma=False,
    )
```

```python
import functools

import jax
import jax.numpy as jnp
from jax import lax
from jax.experimental import pallas as pl
from jax.experimental.pallas import tpu as pltpu
from jax.sharding import PartitionSpec as P

MESH = pl.DeviceIdType.MESH
BF16 = jnp.bfloat16
F32 = jnp.float32
MIB = 1024 * 1024


def dot_nn(a, b):
    return lax.dot_general(a, b, (((1,), (0,)), ((), ())), preferred_element_type=F32)


def flip(t, bit):
    return t + bit - 2 * bit * lax.rem(lax.div(t, bit), 2)


def partner(t, mask):
    bit = 1
    while bit <= mask:
        if mask & bit:
            t = flip(t, bit)
        bit *= 2
    return t


def exchange_kernel(
    ep, tp, cap,
    tok_hbm, og_hbm, routes_hbm, gates_hbm, wg_hbm, wu_hbm, wd_hbm,
    tg_ref, gg_ref, ggo, ugo, dgo,
    tok_ref, og_ref, routes_ref, gates_ref, wg, wu, wd, wgt, wut, wdt, sent, big, comb_ref, pick_ref,
    pg, pu, ph, hid, gp, up, hid_t, gp_t, up_t, dcol,
    psib, rsib, own_sum, pown, rown, tsum, back, dsend, drecv, dsum, dback,
    isem, wsem, out_sem, zr, nr, dr, sr, br, rr, zbr, dtr, dzr,
):
    me_e = lax.axis_index("ep")
    me_t = lax.axis_index("tp")
    core = lax.rem(me_t, 2)
    sib = flip(me_t, 1)
    nbr = (flip(me_t, 2), flip(me_t, 4))
    diag = flip(nbr[0], 4)
    slots = ep * cap
    tok_dev, dw = tok_ref.shape
    fw, model = wg.shape

    def rdma(src, dst, sem, e, t):
        return pltpu.make_async_remote_copy(
            src_ref=src, dst_ref=dst, send_sem=out_sem.at[0], recv_sem=sem,
            device_id={"ep": e, "tp": t}, device_id_type=MESH,
        )

    def arrived(ref, sem):
        rdma(ref, ref, sem, me_e, sib).wait_recv()

    inputs = [
        pltpu.make_async_copy(src, dst, isem.at[i])
        for i, (src, dst) in enumerate((
            (routes_hbm, routes_ref), (gates_hbm, gates_ref), (tok_hbm, tok_ref), (og_hbm, og_ref)))
    ]
    for load in inputs:
        load.start()
    loads = [
        pltpu.make_async_copy(src.at[0], dst, wsem.at[i])
        for i, (src, dst) in enumerate(((wg_hbm, wg), (wu_hbm, wu), (wd_hbm, wd)))
    ]
    barrier = pltpu.get_barrier_semaphore()
    for r in range(1, ep):
        pl.semaphore_signal(
            barrier, inc=1, device_id={"ep": partner(me_e, r), "tp": me_t}, device_id_type=MESH)
    for r in range(1, tp):
        pl.semaphore_signal(
            barrier, inc=1, device_id={"ep": me_e, "tp": partner(me_t, r)}, device_id_type=MESH)

    for load in loads:
        load.start()
    for load in inputs:
        load.wait()

    expert = [routes_ref[k : k + 1, :] for k in range(2)]
    place = [jnp.zeros((1, tok_dev), F32) for _ in range(2)]
    for k in range(2):
        for i in range(ep):
            place[k] = jnp.where(expert[k] == partner(me_e, i), float(i), place[k])
    group = lax.broadcasted_iota(jnp.int32, (16, tok_dev), 0).astype(F32)
    oh = [jnp.where(place[k] == group, 1.0, 0.0) for k in range(2)]
    row_id = lax.broadcasted_iota(jnp.int32, (tok_dev, tok_dev), 0)
    col_id = lax.broadcasted_iota(jnp.int32, (tok_dev, tok_dev), 1)
    above = jnp.where(row_id < col_id, 1.0, 0.0).astype(BF16)
    before = dot_nn((oh[0] + oh[1]).astype(BF16), above)
    rank = [
        jnp.sum(before * oh[0], axis=0, keepdims=True),
        jnp.sum((before + oh[0]) * oh[1], axis=0, keepdims=True),
    ]
    slot_id = lax.broadcasted_iota(jnp.int32, (slots, tok_dev), 0).astype(F32)
    slot_gate = jnp.zeros((slots, 1), F32)
    both = jnp.zeros((slots, tok_dev), F32)
    for k in range(2):
        pick = jnp.where(place[k] * float(cap) + rank[k] == slot_id, 1.0, 0.0)
        pick_ref[k] = pick
        both = both + pick
        slot_gate = slot_gate + jnp.sum(pick * gates_ref[k : k + 1, :], axis=1, keepdims=True)
    select = both.astype(BF16)
    sent[:, 0:dw] = dot_nn(select, tok_ref[...]).astype(BF16)
    sent[:, dw : 2 * dw] = (slot_gate * dot_nn(select, og_ref[...])).astype(BF16)
    big[me_t, 0:cap, :] = sent[0:cap, :]

    pl.semaphore_wait(barrier, ep - 1 + tp - 1)

    sends = []

    def send(src, dst, sem, e, t):
        copy = rdma(src, dst, sem, e, t)
        copy.start()
        sends.append(copy)

    def rows_of(i):
        return pl.ds(i * cap, cap)

    halves = (pl.ds(0, dw), pl.ds(dw, dw))
    direct = (1,)

    def chunk(i, t):
        return big.at[t, rows_of(i)]

    def half(i, t, h):
        return big.at[t, rows_of(i), halves[h]]

    def to_sibling(i, t, far=0):
        send(chunk(i, t), chunk(i, t), sr.at[2 * i + far], me_e, sib)

    def send_z(i):
        return rdma(sent.at[rows_of(i)], big.at[me_t, rows_of(i)], zr.at[i], partner(me_e, i), me_t)

    def stage_a(i):
        if i:
            arrived(chunk(i, me_t), zr.at[i])
        for d in range(2):
            send(chunk(i, me_t), chunk(i, me_t), nr.at[2 * i + d], me_e, nbr[d])
        if i in direct:
            send(chunk(i, me_t), chunk(i, me_t), dr.at[i], me_e, diag)
        to_sibling(i, me_t)

    def stage_b(i):
        for d in range(2):
            arrived(chunk(i, nbr[d]), nr.at[2 * i + d])
            if i not in direct:
                send(half(i, nbr[d], d), half(i, nbr[d], d), dr.at[i], me_e, nbr[1 - d])
        for d in range(2):
            to_sibling(i, nbr[d])

    def stage_c(i):
        arrived(chunk(i, diag), dr.at[i])
        to_sibling(i, diag, 1)

    def settle_near(i):
        arrived(big.at[pl.ds(0, 3), rows_of(i)], sr.at[2 * i])

    def settle_far(i):
        arrived(chunk(i, diag), sr.at[2 * i + 1])

    def turn(w, wt):
        @pl.loop(0, tp)
        def _(j):
            part = pl.ds(pl.multiple_of(j * dw, dw), dw)
            wt[part, :] = w[:, part].T

    lane = lax.broadcasted_iota(jnp.int32, (cap, 128), 1)

    chips = (diag, nbr[0], nbr[1], me_t)

    def product(i, h, wt, some):
        total = None
        for t in some:
            for k in range(2):
                j = lax.div(t, 2) * 2 + k
                term = dot_nn(big[j, rows_of(i), halves[h]], wt[pl.ds(pl.multiple_of(j * dw, dw), dw), :])
                total = term if total is None else total + term
        return total

    def near_x(i):
        pg[...] = product(i, 0, wgt, chips[1:])
        pu[...] = product(i, 0, wut, chips[1:])

    def near_c(i):
        ph[...] = product(i, 1, wdt, chips[1:])

    def forward(i):
        at = rows_of(i)
        g = pg[...] + product(i, 0, wgt, chips[:1])
        u = pu[...] + product(i, 0, wut, chips[:1])
        h = ph[...] + product(i, 1, wdt, chips[:1])
        sig = jax.nn.sigmoid(g)
        act = g * sig
        hidden = (act * u).astype(BF16)
        hid[at, :] = hidden
        gp[at, :] = (h * u * sig * (1.0 + g * (1.0 - sig))).astype(BF16)
        up[at, :] = (h * act).astype(BF16)
        dots = jnp.sum(hidden.astype(F32) * h, axis=1, keepdims=True)
        dcol[0:cap, :] = jnp.where(lane == i, dots, dcol[0:cap, :])

    def pieces(i, lo=0, hi=4):
        at = rows_of(i)
        for q in range(lo, hi):
            wide = pl.ds(pl.multiple_of(lax.div(chips[q], 2) * (2 * dw), 2 * dw), 2 * dw)
            both = dot_nn(gp[at, :], wg[:, wide]) + dot_nn(up[at, :], wu[:, wide])
            low, high = both[:, 0:dw], both[:, dw : 2 * dw]
            psib[i, q] = jnp.where(core == 0, high, low).astype(BF16)
            own_sum[i, q] = jnp.where(core == 0, low, high)
        part = pl.ds(lo, hi - lo)
        send(psib.at[i, part], rsib.at[i, part], br.at[2 * i + (lo > 0)], me_e, sib)

    def spread(i, lo=0, hi=4):
        arrived(rsib.at[i, pl.ds(lo, hi - lo)], br.at[2 * i + (lo > 0)])
        top = min(hi, 3)
        for q in range(lo, top):
            pown[i, q] = (own_sum[i, q] + rsib[i, q].astype(F32)).astype(BF16)
        for q in range(lo, top):
            send(pown.at[i, q], rown.at[i, q], rr.at[i], me_e, chips[q])

    def collect(i):
        arrived(rown.at[i], rr.at[i])
        total = own_sum[i, 3] + rsib[i, 3].astype(F32)
        for q in range(3):
            total = total + rown[i, q].astype(F32)
        if i:
            tsum[rows_of(i), :] = total.astype(BF16)
            send(tsum.at[rows_of(i)], back.at[rows_of(i)], zbr.at[i], partner(me_e, i), me_t)
        else:
            back[rows_of(i), :] = total.astype(BF16)

    def send_dots():
        dsend[...] = dcol[...].T[0:8, :]
        for r in range(1, tp):
            send(dsend, drecv.at[r - 1], dtr.at[0], me_e, partner(me_t, r))

    def return_dots():
        arrived(drecv, dtr.at[0])
        dots = dsend[...]
        for r in range(1, tp):
            dots = dots + drecv[r - 1]
        dsum[...] = dots
        for i in range(1, ep):
            send(dsum, dback.at[i], dzr.at[0], partner(me_e, i), me_t)
        dback[0] = dots

    def weight_grad(rows_t, h, out, lo, hi):
        for k in range(lo, hi):
            out[:, k * dw : (k + 1) * dw] = dot_nn(rows_t[...], big[k, :, halves[h]]).astype(BF16)

    def flats():
        hid_t[...] = hid[...].T
        gp_t[...] = gp[...].T
        up_t[...] = up[...].T

    z_order = (1, 3, 2) if ep == 4 else (1,)
    z_sends = [send_z(i) for i in z_order]
    sends.extend(z_sends)
    z_sends[0].start()
    stage_a(0)
    dcol[...] = jnp.zeros_like(dcol)
    flat = both.T.astype(BF16)
    for i in range(ep):
        comb_ref[i] = flat[:, i * cap : (i + 1) * cap]
    for k, (w, wt) in enumerate(((wg, wgt), (wu, wut), (wd, wdt))):
        loads[k].wait()
        turn(w, wt)
        if k == 0:
            for copy in z_sends[1:]:
                copy.start()
    stage_b(0)
    stage_a(1)
    settle_near(0)
    near_x(0)
    near_c(0)
    stage_c(0)
    if ep == 4:
        stage_a(3)
        stage_b(1)
        stage_a(2)
        settle_far(0)
        forward(0)
        settle_near(1)
        near_x(1)
        stage_c(1)
        near_c(1)
        settle_far(1)
        stage_b(3)
        forward(1)
        stage_b(2)
        pieces(1)
        settle_near(3)
        near_x(3)
        near_c(3)
        stage_c(3)
        spread(1)
        pieces(0)
        settle_far(3)
        forward(3)
        stage_c(2)
        pieces(3)
        spread(0)
        settle_near(2)
        near_x(2)
        settle_far(2)
        spread(3)
        near_c(2)
        forward(2)
        send_dots()
        pieces(2, 0, 2)
        pieces(2, 2, 4)
        collect(1)
        flats()
        spread(2, 0, 2)
        weight_grad(gp_t, 0, ggo, 0, 2)
        spread(2, 2, 4)
        weight_grad(gp_t, 0, ggo, 2, 8)
        collect(3)
        return_dots()
        collect(0)
        weight_grad(up_t, 0, ugo, 0, 8)
        collect(2)
        weight_grad(hid_t, 1, dgo, 0, 8)
        last = 2
    else:
        stage_b(1)
        settle_far(0)
        forward(0)
        stage_c(1)
        settle_near(1)
        near_x(1)
        near_c(1)
        settle_far(1)
        forward(1)
        send_dots()
        pieces(1)
        pieces(0)
        spread(1)
        flats()
        return_dots()
        spread(0)
        weight_grad(gp_t, 0, ggo, 0, 8)
        weight_grad(up_t, 0, ugo, 0, 8)
        collect(1)
        collect(0)
        weight_grad(hid_t, 1, dgo, 0, 8)
        last = 1

    def token_part(i):
        if i:
            arrived(back.at[rows_of(i)], zbr.at[i])
        return dot_nn(comb_ref[i], back[rows_of(i), :])

    arrived(dback.at[pl.ds(1, ep - 1)], dzr.at[0])
    share = tok_dev // tp
    own_row = lax.broadcasted_iota(jnp.int32, (tok_dev, share), 0)
    own_col = lax.broadcasted_iota(jnp.int32, (tok_dev, share), 1) + me_t * share
    own_pick = jnp.where(own_row == own_col, 1.0, 0.0)
    tile_row = lax.broadcasted_iota(jnp.int32, (8, 128), 0)
    held = jnp.zeros((8, 128), F32)
    for i in range(ep):
        held = jnp.where(tile_row == i, dback[i], held)
    held = jnp.concatenate([held, jnp.zeros((120, 128), F32)], axis=0).T
    grads = []
    for k in range(2):
        total = jnp.zeros((1, tok_dev), F32)
        for i in range(ep):
            total = total + jnp.sum(
                held[0:cap, i : i + 1] * pick_ref[k, i * cap : (i + 1) * cap, :], axis=0, keepdims=True)
        grads.append(total / gates_ref[k : k + 1, :])
    shares = jnp.concatenate([*grads, jnp.zeros((6, tok_dev), F32)], axis=0)
    gg_ref[...] = jnp.dot(shares, own_pick, precision=lax.Precision.HIGHEST, preferred_element_type=F32)[0:2, :]

    total = token_part(0)
    for i in range(1, ep):
        if i != last:
            total = total + token_part(i)
    tg_ref[...] = (total + token_part(last)).astype(BF16)
    for copy in sends:
        copy.wait_send()


def store_kernel(tg_ref, gg_ref, gw_ref, uw_ref, dw_ref, tg_out, gg_out, gw_out, uw_out, dw_out, sem):
    copies = [
        pltpu.make_async_copy(src, dst, sem.at[k])
        for k, (src, dst) in enumerate((
            (gw_ref, gw_out.at[0]), (uw_ref, uw_out.at[0]), (dw_ref, dw_out.at[0]),
            (tg_ref, tg_out), (gg_ref, gg_out)))
    ]
    for copy in copies:
        copy.start()
    for copy in copies:
        copy.wait()


def fused(tokens, out_grad, routes, gates, gate_weight, up_weight, down_weight):
    tok_dev, top_k = routes.shape
    ep = lax.axis_size("ep")
    tp = lax.axis_size("tp")
    cap = (3 * tok_dev + ep - 1) // ep
    slots = ep * cap
    dw = tokens.shape[1]
    model = gate_weight.shape[1]
    fw = gate_weight.shape[2]
    share = tok_dev // tp
    vmem = pl.BlockSpec(memory_space=pltpu.VMEM)
    any_ = pl.BlockSpec(memory_space=pl.ANY)
    dma = lambda n: pltpu.SemaphoreType.DMA((n,))
    flops = 16 * slots * model * fw
    small = (((tok_dev, dw), BF16), ((top_k, share), F32))
    grads = (((fw, model), BF16),) * 3
    results = pl.pallas_call(
        functools.partial(exchange_kernel, ep, tp, cap),
        out_shape=tuple(pltpu.VMEM(*leaf) for leaf in small + grads),
        in_specs=[any_] * 7,
        out_specs=[vmem] * 5,
        scratch_shapes=[
            pltpu.VMEM((tok_dev, dw), BF16),
            pltpu.VMEM((tok_dev, dw), BF16),
            pltpu.VMEM((top_k, tok_dev), jnp.int32),
            pltpu.VMEM((top_k, tok_dev), F32),
            pltpu.VMEM((fw, model), BF16),
            pltpu.VMEM((fw, model), BF16),
            pltpu.VMEM((fw, model), BF16),
            pltpu.VMEM((model, fw), BF16),
            pltpu.VMEM((model, fw), BF16),
            pltpu.VMEM((model, fw), BF16),
            pltpu.VMEM((slots, 2 * dw), BF16),
            pltpu.VMEM((tp, slots, 2 * dw), BF16),
            pltpu.VMEM((ep, tok_dev, cap), BF16),
            pltpu.VMEM((2, slots, tok_dev), F32),
            pltpu.VMEM((cap, fw), F32),
            pltpu.VMEM((cap, fw), F32),
            pltpu.VMEM((cap, fw), F32),
            pltpu.VMEM((slots, fw), BF16),
            pltpu.VMEM((slots, fw), BF16),
            pltpu.VMEM((slots, fw), BF16),
            pltpu.VMEM((fw, slots), BF16),
            pltpu.VMEM((fw, slots), BF16),
            pltpu.VMEM((fw, slots), BF16),
            pltpu.VMEM((128, 128), F32),
            pltpu.VMEM((ep, 4, cap, dw), BF16),
            pltpu.VMEM((ep, 4, cap, dw), BF16),
            pltpu.VMEM((ep, 4, cap, dw), F32),
            pltpu.VMEM((ep, 3, cap, dw), BF16),
            pltpu.VMEM((ep, 3, cap, dw), BF16),
            pltpu.VMEM((slots, dw), BF16),
            pltpu.VMEM((slots, dw), BF16),
            pltpu.VMEM((8, 128), F32),
            pltpu.VMEM((tp - 1, 8, 128), F32),
            pltpu.VMEM((8, 128), F32),
            pltpu.VMEM((ep, 8, 128), F32),
            dma(4), dma(3), dma(1), dma(ep), dma(2 * ep), dma(ep), dma(2 * ep), dma(2 * ep), dma(ep), dma(ep),
            dma(1), dma(1),
        ],
        compiler_params=pltpu.CompilerParams(
            collective_id=0, has_side_effects=True, vmem_limit_bytes=46 * MIB),
        cost_estimate=pl.CostEstimate(flops=flops, bytes_accessed=6 * model * fw, transcendentals=0),
    )(tokens, out_grad, routes.T, gates.T, jnp.swapaxes(gate_weight, 1, 2),
      jnp.swapaxes(up_weight, 1, 2), down_weight)
    held = [pltpu.with_memory_space_constraint(r, pltpu.VMEM) for r in results]
    tokens_grad, gates_grad, gate_grad, up_grad, down_grad = pl.pallas_call(
        store_kernel,
        out_shape=tuple(jax.ShapeDtypeStruct(*leaf) for leaf in small)
        + tuple(jax.ShapeDtypeStruct((1, *shape), dtype) for shape, dtype in grads),
        in_specs=[vmem] * 5,
        out_specs=[any_] * 5,
        scratch_shapes=[dma(5)],
        compiler_params=pltpu.CompilerParams(vmem_limit_bytes=16 * MIB),
        cost_estimate=pl.CostEstimate(flops=slots * fw, bytes_accessed=6 * model * fw, transcendentals=0),
    )(*held)
    return (tokens_grad, gates_grad.T, jnp.swapaxes(gate_grad, 1, 2), jnp.swapaxes(up_grad, 1, 2), down_grad)


def fits_fused(ep, tp, tokens, routes, gate_weight):
    cap = (3 * routes.shape[0] + ep - 1) // ep
    return (
        tp == 8 and ep in (2, 4) and cap % 16 == 0 and cap <= 128
        and tokens.shape[1] % 128 == 0 and routes.shape[1] == 2
        and routes.shape[0] == 128
        and gate_weight.shape[2] % 16 == 0
    )


def expert_grads(rows, cotan, w_gate, w_up, w_down):
    pre_gate = jnp.dot(rows, w_gate, preferred_element_type=jnp.float32)
    pre_up = jnp.dot(rows, w_up, preferred_element_type=jnp.float32)
    activated = jax.nn.silu(pre_gate)
    hidden = (activated * pre_up).astype(jnp.bfloat16)
    hid_grad = jnp.dot(cotan, w_down.T, preferred_element_type=jnp.float32)
    sigmoid_gate = jax.nn.sigmoid(pre_gate)
    gate_part = (hid_grad * pre_up * sigmoid_gate * (1.0 + pre_gate * (1.0 - sigmoid_gate))).astype(
        jnp.bfloat16
    )
    up_part = (hid_grad * activated).astype(jnp.bfloat16)
    slot_dots = jnp.sum(hidden.astype(jnp.float32) * hid_grad, axis=1)
    down_grad = jnp.dot(hidden.T, cotan, preferred_element_type=jnp.float32).astype(jnp.bfloat16)
    gate_grad = jnp.dot(rows.T, gate_part, preferred_element_type=jnp.float32).astype(jnp.bfloat16)
    up_grad = jnp.dot(rows.T, up_part, preferred_element_type=jnp.float32).astype(jnp.bfloat16)
    return (gate_part, up_part, slot_dots, gate_grad, up_grad, down_grad)


def on_device(tokens, out_grad, routes, gates, gate_weight, up_weight, down_weight):
    tok_dev, top_k = routes.shape
    ep_size = lax.axis_size("ep")
    tp_size = lax.axis_size("tp")
    if fits_fused(ep_size, tp_size, tokens, routes, gate_weight):
        return fused(tokens, out_grad, routes, gates, gate_weight, up_weight, down_weight)
    capacity = (3 * tok_dev + ep_size - 1) // ep_size
    buffer_rows = ep_size * capacity
    slice_width = tokens.shape[1]
    flat_expert = routes.reshape(-1)
    onehot = (flat_expert[:, None] == jnp.arange(ep_size, dtype=jnp.int32)[None, :]).astype(
        jnp.int32
    )
    slot_rank = jnp.sum((jnp.cumsum(onehot, axis=0) - onehot) * onehot, axis=1)
    slot_dest = flat_expert * capacity + slot_rank
    placed = jnp.arange(buffer_rows, dtype=jnp.int32)[:, None] == slot_dest[None, :]
    placed_float = placed.astype(jnp.float32)
    select = jnp.any(placed.reshape(buffer_rows, tok_dev, top_k), axis=2).astype(jnp.bfloat16)
    slot_gate = jnp.dot(placed_float, gates.reshape(-1), precision=lax.Precision.HIGHEST)
    sent_rows = jnp.dot(select, tokens, preferred_element_type=jnp.float32).astype(jnp.bfloat16)
    cotan_rows = jnp.dot(select, out_grad, preferred_element_type=jnp.float32)
    sent_cotan = (slot_gate[:, None] * cotan_rows).astype(jnp.bfloat16)
    recv_rows, recv_cotan = (
        lax.all_to_all(
            sent_rows.reshape(ep_size, capacity, slice_width),
            "ep",
            split_axis=0,
            concat_axis=0,
            tiled=True,
        ),
        lax.all_to_all(
            sent_cotan.reshape(ep_size, capacity, slice_width),
            "ep",
            split_axis=0,
            concat_axis=0,
            tiled=True,
        ),
    )
    whole_rows, whole_cotan = (
        lax.all_gather(recv_rows, "tp", axis=2, tiled=True),
        lax.all_gather(recv_cotan, "tp", axis=2, tiled=True),
    )
    model_width = whole_rows.shape[2]
    rows = whole_rows.reshape(buffer_rows, model_width)
    cotan = whole_cotan.reshape(buffer_rows, model_width)
    w_gate = gate_weight[0]
    w_up = up_weight[0]
    gate_part, up_part, slot_dots, gate_grad, up_grad, down_grad = expert_grads(
        rows, cotan, w_gate, w_up, down_weight[0]
    )
    partial_value = jnp.dot(gate_part, w_gate.T, preferred_element_type=jnp.float32)
    partial_value = (
        partial_value + jnp.dot(up_part, w_up.T, preferred_element_type=jnp.float32)
    ).astype(jnp.bfloat16)
    share = tok_dev // tp_size
    start = lax.axis_index("tp") * share
    summed = lax.psum(slot_dots, "tp")
    row_sums = lax.psum_scatter(
        partial_value.reshape(ep_size, capacity, model_width), "tp", scatter_dimension=2, tiled=True
    ).astype(jnp.float32)
    back_rows, back_dots = (
        lax.all_to_all(
            row_sums.astype(jnp.bfloat16), "ep", split_axis=0, concat_axis=0, tiled=True
        ).astype(row_sums.dtype),
        lax.all_to_all(
            summed.reshape(ep_size, capacity).astype(jnp.bfloat16),
            "ep",
            split_axis=0,
            concat_axis=0,
            tiled=True,
        ).astype(jnp.float32),
    )
    slot_rows = back_rows.reshape(buffer_rows, slice_width)[slot_dest]
    tokens_grad = jnp.sum(slot_rows.reshape(tok_dev, top_k, slice_width), axis=1).astype(
        jnp.bfloat16
    )
    token_dots = back_dots.reshape(buffer_rows)[slot_dest].reshape(tok_dev, top_k)
    own_dots = lax.dynamic_slice_in_dim(token_dots, start, share, 0)
    own_gates = lax.dynamic_slice_in_dim(gates, start, share, 0)
    gates_grad = own_dots / own_gates
    return (tokens_grad, gates_grad, gate_grad[None], up_grad[None], down_grad[None])


def solution(mesh):
    placed = (
        P("ep", "tp"),
        P("ep", "tp"),
        P("ep", None),
        P("ep", None),
        P("ep", None, "tp"),
        P("ep", None, "tp"),
        P("ep", "tp", None),
    )
    return jax.shard_map(
        on_device,
        mesh=mesh,
        in_specs=placed,
        out_specs=(
            P("ep", "tp"),
            P(("ep", "tp"), None),
            P("ep", None, "tp"),
            P("ep", None, "tp"),
            P("ep", "tp", None),
        ),
        check_vma=False,
    )
```
